32 devices in a mesh: sp: 16 (over z, y, x), tp: 2 (over core).
Axes of the slice: x: 2, y: 2, z: 4, core: 2. Of those that a mesh axis runs over, the one named last changes fastest.
Arguments:
- latent: bfloat16 [4096, 2048], P('sp'), may hold values from -6 to 6
- context: bfloat16 [512, 2048], P('sp'), may hold values from -6 to 6
- cond: bfloat16 [2048], P('sp'), may hold values from -6 to 6
- cond_ctx: bfloat16 [2048], P('sp'), may hold values from -6 to 6
- shift_weight: bfloat16 [2048, 2048], P('sp', 'tp'), may hold values from -0.125 to 0.125
- scale_weight: bfloat16 [2048, 2048], P('sp', 'tp'), may hold values from -0.125 to 0.125
- gate_weight: bfloat16 [2048, 2048], P('sp', 'tp'), may hold values from -0.25 to 0.25
- norm_gain: bfloat16 [2048], replicated, may hold values from 0.099609375 to 1.8984375
- query_weight: bfloat16 [2048, 1024], P(None, 'tp'), may hold values from -0.125 to 0.125
- key_weight: bfloat16 [2048, 1024], P(None, 'tp'), may hold values from -0.125 to 0.125
- value_weight: bfloat16 [2048, 1024], P(None, 'tp'), may hold values from -0.125 to 0.125
- query_gain: bfloat16 [64], replicated, may hold values from 0.099609375 to 1.8984375
- key_gain: bfloat16 [64], replicated, may hold values from 0.099609375 to 1.8984375
- offset_bias: float32 [16, 15, 31], P('tp'), may hold values from -0.5 to 251
- out_weight: bfloat16 [1024, 2048], P(None, 'tp'), may hold values from -1.5 to 1.5
Outputs:
- updated: bfloat16 [4096, 2048], P('sp', 'tp')
The draws below stay inside these ranges and needn't reach their ends.
All inputs are finite; a program needn't handle non-finite values.
Results may differ from the reference program's by a relative error of at most 0.0077.
Values may be sent and summed in bfloat16 or wider, within the bound.
A program may use at most 128 MiB of HBM per device.

```python
import jax
import jax.numpy as jnp
from jax import lax

D = 2048
HEADS = 16
HEAD_DIM = 64
WIN_ROWS = 8
WIN_COLS = 16
GRID_W = 64
CTX = 512
TOKENS = 4096
HD = 1024


def draw_offset_bias(key, part):
    shape = (HEADS, 2 * WIN_ROWS - 1, 2 * WIN_COLS - 1)
    table = jax.random.uniform(jax.random.fold_in(key, 11), shape, jnp.float32, -0.5, 1.0)
    return table


def block_levels(rng, extent, cuts, low, largest):
    def one(position, shards_of):
        heights = jax.random.uniform(jax.random.fold_in(jax.random.fold_in(rng, 6), position), (shards_of,), jnp.float32, low / len(cuts), largest / len(cuts))
        return jnp.repeat(jnp.exp(heights), extent[position] // shards_of).reshape((-1,) + (1,) * (len(extent) - position - 1))

    factor_of = one(*cuts[0])
    for cut in cuts[1:]:
        factor_of = factor_of * one(*cut)
    return factor_of


def gaussian(key, dims, width, limit, shards=(), kind=jnp.bfloat16):
    level = block_levels(key, dims, shards, -0.22, 0.18) if shards else 1.0
    entries = jax.random.normal(key, dims, jnp.float32) * width * level
    return jnp.minimum(jnp.maximum(entries, -limit), limit).astype(kind)


def setup_inputs(seed: int = 0) -> dict:
    splits = jax.random.split(jax.random.key(seed), 16)
    latent = gaussian(splits[0], (TOKENS, D), 1.0, 6.0, ((0, 16),))
    context = gaussian(splits[1], (CTX, D), 1.0, 6.0, ((0, 16),))
    cond = gaussian(splits[2], (D,), 1.0, 6.0, ((0, 16),))
    cond_ctx = gaussian(splits[3], (D,), 1.0, 6.0, ((0, 16),))
    shift_weight = gaussian(splits[4], (D, D), D ** -0.5, 0.125, ((0, 16), (1, 2)))
    scale_weight = gaussian(splits[5], (D, D), D ** -0.5, 0.125, ((0, 16), (1, 2)))
    gate_weight = gaussian(splits[6], (D, D), (D // 4) ** -0.5, 0.25, ((0, 16), (1, 2)))
    norm_gain = jnp.clip(1.0 + 0.18 * jax.random.normal(splits[7], (D,), jnp.float32), 0.099609375, 1.8984375).astype(jnp.bfloat16)
    query_weight = gaussian(splits[8], (D, HD), D ** -0.5, 0.125, ((1, 2),))
    key_weight = gaussian(splits[9], (D, HD), D ** -0.5, 0.125, ((1, 2),))
    value_weight = gaussian(splits[10], (D, HD), D ** -0.5, 0.125, ((1, 2),))
    query_gain = jnp.clip(1.0 + 0.18 * jax.random.normal(splits[11], (HEAD_DIM,), jnp.float32), 0.099609375, 1.8984375).astype(jnp.bfloat16)
    key_gain = jnp.clip(1.0 + 0.18 * jax.random.normal(splits[12], (HEAD_DIM,), jnp.float32), 0.099609375, 1.8984375).astype(jnp.bfloat16)
    offset_bias = draw_offset_bias(jax.random.fold_in(splits[15], 71), 0)
    out_weight = gaussian(splits[14], (HD, D), (max(HD // 64, 1)) ** -0.5, 1.5, ((1, 2),))
    return {"latent": latent, "context": context, "cond": cond, "cond_ctx": cond_ctx, "shift_weight": shift_weight, "scale_weight": scale_weight, "gate_weight": gate_weight, "norm_gain": norm_gain, "query_weight": query_weight, "key_weight": key_weight, "value_weight": value_weight, "query_gain": query_gain, "key_gain": key_gain, "offset_bias": offset_bias, "out_weight": out_weight}


EPS = 1e-06

def modulate(rows, norm_gain, scale, shift):
    values = rows.astype(jnp.float32)
    normed = values * lax.rsqrt(lax.optimization_barrier(jnp.mean(values * values, axis=-1, keepdims=True)) + EPS)
    return (normed * norm_gain.astype(jnp.float32) * (1.0 + scale) + shift).astype(jnp.bfloat16)

def project_heads(hidden, weight, gain):
    raw = jnp.dot(hidden, weight, preferred_element_type=jnp.float32)
    split = raw.reshape(hidden.shape[0], -1, HEAD_DIM)
    if gain is None:
        return split.astype(jnp.bfloat16)
    normed = split * lax.rsqrt(lax.optimization_barrier(jnp.mean(split * split, axis=-1, keepdims=True)) + EPS)
    return (normed * gain.astype(jnp.float32)).astype(jnp.bfloat16)

def reference(latent, context, cond, cond_ctx, shift_weight, scale_weight, gate_weight, norm_gain, query_weight, key_weight, value_weight, query_gain, key_gain, offset_bias, out_weight):
    act = jax.nn.silu(cond.astype(jnp.float32)).astype(jnp.bfloat16)[None, :]
    act_ctx = jax.nn.silu(cond_ctx.astype(jnp.float32)).astype(jnp.bfloat16)[None, :]
    shift = jnp.dot(act, shift_weight, preferred_element_type=jnp.float32)[0]
    scale = jnp.dot(act, scale_weight, preferred_element_type=jnp.float32)[0]
    gate = jnp.dot(act, gate_weight, preferred_element_type=jnp.float32)[0]
    shift_ctx = jnp.dot(act_ctx, shift_weight, preferred_element_type=jnp.float32)[0]
    scale_ctx = jnp.dot(act_ctx, scale_weight, preferred_element_type=jnp.float32)[0]
    hidden = modulate(latent, norm_gain, scale, shift)
    queries = project_heads(hidden, query_weight, query_gain)
    keys = project_heads(hidden, key_weight, key_gain)
    values = project_heads(hidden, value_weight, None)
    hidden_ctx = modulate(context, norm_gain, scale_ctx, shift_ctx)
    ctx_keys = project_heads(hidden_ctx, key_weight, key_gain).astype(jnp.float32)
    ctx_values = project_heads(hidden_ctx, value_weight, None).astype(jnp.float32)
    total_rows = latent.shape[0] // GRID_W
    grid_q = queries.reshape(total_rows, GRID_W, HEADS, HEAD_DIM)
    grid_k = keys.reshape(total_rows, GRID_W, HEADS, HEAD_DIM)
    grid_v = values.reshape(total_rows, GRID_W, HEADS, HEAD_DIM)
    column = jnp.arange(GRID_W, dtype=jnp.int32)
    window_first = jnp.clip(column - WIN_COLS // 2, 0, GRID_W - WIN_COLS)
    inside = (column[None, :] >= window_first[:, None]) & (column[None, :] < window_first[:, None] + WIN_COLS)
    col_offset = jnp.clip(column[None, :] - column[:, None] + WIN_COLS - 1, 0, 2 * WIN_COLS - 2)
    by_col = offset_bias.astype(jnp.float32)[:, :, col_offset]
    factor = HEAD_DIM ** (-0.5)
    band_len = WIN_ROWS * GRID_W

    def one_row(row):
        first = jnp.clip(row - WIN_ROWS // 2, 0, total_rows - WIN_ROWS).astype(jnp.int32)
        band_k = lax.dynamic_slice_in_dim(grid_k, first, WIN_ROWS, 0).astype(jnp.float32)
        band_v = lax.dynamic_slice_in_dim(grid_v, first, WIN_ROWS, 0).astype(jnp.float32)
        query = lax.dynamic_index_in_dim(grid_q, row, 0, keepdims=False).astype(jnp.float32)
        row_offset = (first + jnp.arange(WIN_ROWS, dtype=jnp.int32) - row + WIN_ROWS - 1).astype(jnp.int32)
        bias = jnp.take(by_col, row_offset, axis=1)
        scores = jnp.einsum('qhd,jkhd->hqjk', query, band_k) * factor + jnp.transpose(bias, (0, 2, 1, 3))
        scores = jnp.where(inside[None, :, None, :], scores, -jnp.inf).reshape(HEADS, GRID_W, band_len)
        ctx_scores = jnp.einsum('qhd,chd->hqc', query, ctx_keys) * factor
        weights = jax.nn.softmax(jnp.concatenate([scores, ctx_scores], axis=-1), axis=-1).astype(jnp.bfloat16)
        weights = lax.optimization_barrier(weights).astype(jnp.float32)
        local_w = weights[..., :band_len].reshape(HEADS, GRID_W, WIN_ROWS, GRID_W)
        mixed = jnp.einsum('hqjk,jkhd->qhd', local_w, band_v) + jnp.einsum('hqc,chd->qhd', weights[..., band_len:], ctx_values)
        return mixed.astype(jnp.bfloat16).reshape(GRID_W, HEADS * HEAD_DIM)
    mixed = lax.map(one_row, jnp.arange(total_rows, dtype=jnp.int32)).reshape(latent.shape[0], HEADS * HEAD_DIM)
    projected = jnp.dot(mixed, out_weight, preferred_element_type=jnp.float32)
    return (latent.astype(jnp.float32) + gate[None, :] * projected).astype(jnp.bfloat16)
```

```python
import functools

import jax
import jax.numpy as jnp
import numpy as np
from jax import lax
from jax.experimental import pallas as pl
from jax.experimental.pallas import tpu as pltpu
from jax.sharding import PartitionSpec as P

HEAD_DIM = 64
WIN_ROWS = 8
WIN_COLS = 16
GRID_W = 64


EPS = 1e-06


def padded_2(block, sides, width):
    for axis, dim in sides:
        count = lax.axis_size(axis)
        forward = [(i, i + 1) for i in range(count - 1)]
        backward = [(target, source) for source, target in forward]
        low = lax.ppermute(
            lax.slice_in_dim(block, block.shape[dim] - width, None, axis=dim), axis, forward
        )
        high = lax.ppermute(lax.slice_in_dim(block, 0, width, axis=dim), axis, backward)
        block = jnp.concatenate([low, block, high], axis=dim)
    return block


def modulate(rows, norm_gain, scale, shift):
    values = rows.astype(jnp.float32)
    normed = values * lax.rsqrt(jnp.mean(values * values, axis=-1, keepdims=True) + EPS)
    return (normed * norm_gain.astype(jnp.float32) * (1.0 + scale) + shift).astype(jnp.bfloat16)


def project_heads(hidden, weight, gain):
    raw = jnp.dot(hidden, weight, preferred_element_type=jnp.float32)
    split = raw.reshape(hidden.shape[0], -1, HEAD_DIM)
    if gain is None:
        return split.astype(jnp.bfloat16)
    normed = split * lax.rsqrt(jnp.mean(split * split, axis=-1, keepdims=True) + EPS)
    return (normed * gain.astype(jnp.float32)).astype(jnp.bfloat16)


def body(
    latent,
    context,
    cond,
    cond_ctx,
    shift_weight,
    scale_weight,
    gate_weight,
    norm_gain,
    query_weight,
    key_weight,
    value_weight,
    query_gain,
    key_gain,
    offset_bias,
    out_weight,
):
    width = latent.shape[1]
    col_width = shift_weight.shape[1]
    tp_offset = lax.axis_index("tp") * col_width
    act = jax.nn.silu(cond.astype(jnp.float32)).astype(jnp.bfloat16)
    act_ctx = jax.nn.silu(cond_ctx.astype(jnp.float32)).astype(jnp.bfloat16)
    acts = jnp.stack([act, act_ctx])
    terms = jnp.concatenate(
        [
            jnp.dot(acts, shift_weight, preferred_element_type=jnp.float32),
            jnp.dot(acts, scale_weight, preferred_element_type=jnp.float32),
            jnp.dot(acts[:1], gate_weight, preferred_element_type=jnp.float32),
        ],
        axis=0,
    )
    placed = lax.dynamic_update_slice_in_dim(
        jnp.zeros((5, width), jnp.float32), terms, tp_offset, 1
    )
    full = lax.psum(placed, ("sp", "tp"))
    shift, shift_ctx, scale, scale_ctx, gate = (full[0], full[1], full[2], full[3], full[4])
    heads_dev = offset_bias.shape[0]
    lane = heads_dev * HEAD_DIM
    all_rows = lax.all_gather(context, "sp", axis=0, tiled=True)
    hidden_ctx = modulate(all_rows, norm_gain, scale_ctx, shift_ctx)
    ctx_keys = project_heads(hidden_ctx, key_weight, key_gain)
    ctx_values = project_heads(hidden_ctx, value_weight, None)
    hidden = modulate(latent, norm_gain, scale, shift)
    queries = project_heads(hidden, query_weight, query_gain)
    keys = project_heads(hidden, key_weight, key_gain)
    values = project_heads(hidden, value_weight, None)
    rows_dev = latent.shape[0] // GRID_W
    reach = WIN_ROWS // 2
    grid_kv = jnp.stack(
        [keys.reshape(rows_dev, GRID_W, lane), values.reshape(rows_dev, GRID_W, lane)], axis=1
    )
    padded = padded_2(grid_kv, (("sp", 0),), reach)
    total_rows = rows_dev * lax.axis_size("sp")
    base = lax.axis_index("sp") * rows_dev
    local_rows = base + jnp.arange(rows_dev, dtype=jnp.int32)
    first = jnp.clip(local_rows - reach, 0, total_rows - WIN_ROWS)
    window_rows = jnp.arange(WIN_ROWS, dtype=jnp.int32)
    band_index = (first - base + reach)[:, None] + window_rows[None, :]
    band = jnp.take(padded, band_index, axis=0)
    n_blocks = GRID_W // WIN_COLS
    span = 2 * WIN_COLS
    starts = [
        min(max(block * WIN_COLS - WIN_COLS // 2, 0), GRID_W - span) for block in range(n_blocks)
    ]
    blocked = jnp.stack([band[:, :, :, begin : begin + span] for begin in starts], axis=3)
    blocked = blocked.reshape(rows_dev, WIN_ROWS, 2, n_blocks, span, heads_dev, HEAD_DIM)
    key_blocks = blocked[:, :, 0]
    value_blocks = blocked[:, :, 1]
    query_col = np.arange(n_blocks)[:, None, None] * WIN_COLS + np.arange(WIN_COLS)[None, :, None]
    key_col = np.array(starts)[:, None, None] + np.arange(span)[None, None, :]
    window_first = np.clip(query_col - WIN_COLS // 2, 0, GRID_W - WIN_COLS)
    inside = (key_col >= window_first) & (key_col < window_first + WIN_COLS)
    col_offset = np.clip(key_col - query_col + WIN_COLS - 1, 0, 2 * WIN_COLS - 2)
    col_onehot = (col_offset[..., None] == np.arange(2 * WIN_COLS - 1)).astype(np.float32)
    row_offset = first[:, None] + window_rows[None, :] - local_rows[:, None] + WIN_ROWS - 1
    row_onehot = (row_offset[..., None] == jnp.arange(2 * WIN_ROWS - 1, dtype=jnp.int32)).astype(
        jnp.float32
    )
    by_col = jnp.einsum(
        "hxc,bqkc->hxbqk", offset_bias, jnp.asarray(col_onehot), precision=lax.Precision.HIGHEST
    )
    bias = jnp.einsum("rjx,hxbqk->rhbqjk", row_onehot, by_col, precision=lax.Precision.HIGHEST)
    factor = HEAD_DIM ** (-0.5)
    grid_q = queries.reshape(rows_dev, n_blocks, WIN_COLS, heads_dev, HEAD_DIM)
    local_scores = (
        jnp.einsum("rbqhd,rjbkhd->rhbqjk", grid_q, key_blocks, preferred_element_type=jnp.float32)
        * factor
    )
    local_scores = jnp.where(jnp.asarray(inside)[:, :, None, :], local_scores + bias, -jnp.inf)
    band_len = WIN_ROWS * span
    local_scores = local_scores.reshape(rows_dev, heads_dev, n_blocks, WIN_COLS, band_len)
    ctx_scores = (
        jnp.einsum("rbqhd,chd->rhbqc", grid_q, ctx_keys, preferred_element_type=jnp.float32)
        * factor
    )
    scores = jnp.concatenate([local_scores, ctx_scores], axis=-1)
    top = jnp.max(scores, axis=-1, keepdims=True)
    expd = jnp.exp(scores - top)
    weights = (expd / jnp.sum(expd, axis=-1, keepdims=True)).astype(jnp.bfloat16)
    local_w = weights[..., :band_len].reshape(
        rows_dev, heads_dev, n_blocks, WIN_COLS, WIN_ROWS, span
    )
    mixed = jnp.einsum(
        "rhbqjk,rjbkhd->rbqhd", local_w, value_blocks, preferred_element_type=jnp.float32
    )
    mixed = mixed + jnp.einsum(
        "rhbqc,chd->rbqhd", weights[..., band_len:], ctx_values, preferred_element_type=jnp.float32
    )
    mixed = mixed.astype(jnp.bfloat16).reshape(latent.shape[0], lane)
    projected = jnp.dot(
        lax.all_gather(mixed, "tp", axis=1, tiled=True),
        out_weight,
        preferred_element_type=jnp.float32,
    )
    own_cols = lax.dynamic_slice_in_dim(latent, tp_offset, col_width, 1).astype(jnp.float32)
    gate_cols = lax.dynamic_slice_in_dim(gate, tp_offset, col_width, 0)
    return (own_cols + gate_cols[None, :] * projected).astype(jnp.bfloat16)


LANES = 128
NEG = -1e30


def head_norm(raw, gain, ones):
    square = raw * raw
    high = square.astype(jnp.bfloat16)
    low = (square - high.astype(jnp.float32)).astype(jnp.bfloat16)
    parts = []
    for begin in range(0, raw.shape[1], LANES):
        cut = slice(begin, begin + LANES)
        parts.append(
            jnp.dot(high[:, cut], ones, preferred_element_type=jnp.float32)
            + jnp.dot(low[:, cut], ones, preferred_element_type=jnp.float32)
        )
    mean = jnp.concatenate(parts, axis=1) * (1.0 / HEAD_DIM)
    return raw * lax.rsqrt(mean + EPS) * gain


def attend_kernel(
    total_rows,
    low_ref,
    own_ref,
    high_ref,
    ctx_ref,
    mod_ref,
    norm_gain_ref,
    wq_ref,
    wk_ref,
    wv_ref,
    query_gain_ref,
    key_gain_ref,
    table_ref,
    out_ref,
    q_buf,
    k_buf,
    v_buf,
    ck_buf,
    cv_buf,
    low_vmem,
    own_vmem,
    high_vmem,
    ctx_vmem,
    wq_vmem,
    wk_vmem,
    wv_vmem,
    sems,
):
    tokens, lane = out_ref.shape
    streams = {}
    for place, (name, source, target) in enumerate(
        (
            ("own", own_ref, own_vmem),
            ("wk", wk_ref, wk_vmem),
            ("wv", wv_ref, wv_vmem),
            ("wq", wq_ref, wq_vmem),
            ("low", low_ref, low_vmem),
            ("high", high_ref, high_vmem),
            ("ctx", ctx_ref, ctx_vmem),
        )
    ):
        streams[name] = pltpu.make_async_copy(source, target, sems.at[place])
        streams[name].start()
    rows_dev = tokens // GRID_W
    reach = WIN_ROWS // 2
    halo = reach * GRID_W
    heads = lane // HEAD_DIM
    norm_gain = norm_gain_ref[...].astype(jnp.float32)
    half = lax.broadcasted_iota(jnp.int32, (LANES, LANES), 0) // HEAD_DIM
    half_t = lax.broadcasted_iota(jnp.int32, (LANES, LANES), 1) // HEAD_DIM
    ones = (half == half_t).astype(jnp.float32).astype(jnp.bfloat16)
    query_gain = jnp.concatenate([query_gain_ref[...].astype(jnp.float32)] * heads, axis=1)
    key_gain = jnp.concatenate([key_gain_ref[...].astype(jnp.float32)] * heads, axis=1)

    def hidden_of(x, shift, scale):
        values = x.astype(jnp.float32)
        inv = lax.rsqrt(jnp.mean(values * values, axis=-1, keepdims=True) + EPS)
        return (values * inv * (norm_gain * (1.0 + scale)) + shift).astype(jnp.bfloat16)

    def keys_values(hidden, k_out, v_out, at):
        raw = jnp.dot(hidden, wk_vmem[...], preferred_element_type=jnp.float32)
        k_out[pl.ds(at, hidden.shape[0]), :] = head_norm(raw, key_gain, ones).astype(jnp.bfloat16)
        v_out[pl.ds(at, hidden.shape[0]), :] = jnp.dot(
            hidden, wv_vmem[...], preferred_element_type=jnp.float32
        ).astype(jnp.bfloat16)

    shift, shift_ctx = mod_ref[0:1, :], mod_ref[1:2, :]
    scale, scale_ctx = mod_ref[2:3, :], mod_ref[3:4, :]
    step = min(256, tokens)
    streams["own"].wait()
    for begin in range(0, tokens, step):
        hidden = hidden_of(own_vmem[begin : begin + step, :], shift, scale)
        if begin == 0:
            streams["wk"].wait()
            streams["wv"].wait()
        keys_values(hidden, k_buf, v_buf, halo + begin)
        if begin == 0:
            streams["wq"].wait()
        raw = jnp.dot(hidden, wq_vmem[...], preferred_element_type=jnp.float32)
        q_buf[begin : begin + step, :] = (
            head_norm(raw, query_gain, ones).astype(jnp.bfloat16) * HEAD_DIM ** (-0.5)
        ).astype(jnp.bfloat16)
    streams["low"].wait()
    keys_values(hidden_of(low_vmem[...], shift, scale), k_buf, v_buf, 0)
    streams["high"].wait()
    keys_values(hidden_of(high_vmem[...], shift, scale), k_buf, v_buf, halo + tokens)
    ctx_step = min(256, ctx_vmem.shape[0])
    streams["ctx"].wait()

    @pl.loop(0, ctx_vmem.shape[0] // ctx_step)
    def _(block):
        at = pl.multiple_of(block * ctx_step, ctx_step)
        hidden = hidden_of(ctx_vmem[pl.ds(at, ctx_step), :], shift_ctx, scale_ctx)
        keys_values(hidden, ck_buf, cv_buf, at)

    base = lax.axis_index("sp") * rows_dev
    query_col = lax.broadcasted_iota(jnp.int32, (GRID_W, LANES), 0)
    lane_at = lax.broadcasted_iota(jnp.int32, (GRID_W, LANES), 1)
    key_col = lane_at % GRID_W
    window_first = jnp.clip(query_col - WIN_COLS // 2, 0, GRID_W - WIN_COLS)
    inside = (key_col >= window_first) & (key_col < window_first + WIN_COLS)
    first_head = lane_at < HEAD_DIM
    per_tile = LANES // GRID_W
    contract = (((1,), (1,)), ((), ()))

    @pl.loop(0, lane // LANES)
    def _(pair):
        cols = pl.ds(pl.multiple_of(pair * LANES, LANES), LANES)
        for row in range(rows_dev):
            first = jnp.clip(base + row - reach, 0, total_rows - WIN_ROWS)
            begin = pl.multiple_of((first - base + reach) * GRID_W, GRID_W)
            offset = first - base - row + WIN_ROWS - 1
            mine = slice(row * GRID_W, (row + 1) * GRID_W)
            query = q_buf[mine, cols]
            zero = jnp.zeros_like(query)
            query2 = jnp.concatenate(
                [jnp.where(first_head, query, zero), jnp.where(first_head, zero, query)], axis=0
            )
            band = pl.ds(begin, WIN_ROWS * GRID_W)
            local = lax.dot_general(
                query2, k_buf[band, cols], contract, preferred_element_type=jnp.float32
            )
            ctx = lax.dot_general(
                query2, ck_buf[:, cols], contract, preferred_element_type=jnp.float32
            )
            biases = []
            for head in range(2):
                tiles = []
                for tile in range(WIN_ROWS // per_tile):
                    entry = (pair * 2 + head) * (2 * WIN_ROWS) + offset + tile * per_tile
                    line = jnp.broadcast_to(table_ref[entry], (GRID_W, LANES))
                    moved = pltpu.roll(line, LANES - (WIN_COLS - 1), 1, stride=1, stride_axis=0)
                    tiles.append(jnp.where(inside, moved, NEG))
                biases.append(jnp.concatenate(tiles, axis=1))
            local = local + jnp.concatenate(biases, axis=0)
            top = jnp.maximum(
                jnp.max(local, axis=-1, keepdims=True), jnp.max(ctx, axis=-1, keepdims=True)
            )
            local = jnp.exp(local - top)
            ctx = jnp.exp(ctx - top)
            total = jnp.sum(local, axis=-1, keepdims=True) + jnp.sum(ctx, axis=-1, keepdims=True)
            mixed = jnp.dot(
                local.astype(jnp.bfloat16), v_buf[band, cols], preferred_element_type=jnp.float32
            ) + jnp.dot(
                ctx.astype(jnp.bfloat16), cv_buf[:, cols], preferred_element_type=jnp.float32
            )
            mixed = mixed / total
            out_ref[mine, cols] = jnp.where(
                first_head, mixed[:GRID_W], mixed[GRID_W:]
            ).astype(jnp.bfloat16)


def bias_lines(offset_bias):
    heads = offset_bias.shape[0]
    wide = jnp.pad(offset_bias, ((0, 0), (0, 2), (0, GRID_W - offset_bias.shape[2])))
    lines = jnp.concatenate([wide[:, :-1], wide[:, 1:]], axis=2)
    return lines.reshape(heads * 2 * WIN_ROWS, 1, LANES)


def attend(
    low, own, high, ctx, mod, norm_gain, wq, wk, wv, query_gain, key_gain, offset_bias, total_rows
):
    tokens, lane = own.shape[0], wq.shape[1]
    halo = low.shape[0]
    rows = tokens + 2 * halo
    vmem = pl.BlockSpec(memory_space=pltpu.VMEM)
    hbm = pl.BlockSpec(memory_space=pl.ANY)
    return pl.pallas_call(
        functools.partial(attend_kernel, total_rows),
        out_shape=jax.ShapeDtypeStruct((tokens, lane), jnp.bfloat16),
        in_specs=[hbm] * 4 + [vmem] * 2 + [hbm] * 3 + [vmem] * 3,
        out_specs=vmem,
        scratch_shapes=[
            pltpu.VMEM((tokens, lane), jnp.bfloat16),
            pltpu.VMEM((rows, lane), jnp.bfloat16),
            pltpu.VMEM((rows, lane), jnp.bfloat16),
            pltpu.VMEM((ctx.shape[0], lane), jnp.bfloat16),
            pltpu.VMEM((ctx.shape[0], lane), jnp.bfloat16),
        ]
        + [pltpu.VMEM(x.shape, x.dtype) for x in (low, own, high, ctx, wq, wk, wv)]
        + [pltpu.SemaphoreType.DMA((7,))],
        cost_estimate=pl.CostEstimate(
            flops=12 * tokens * own.shape[1] * lane, bytes_accessed=1 << 24, transcendentals=1 << 21
        ),
        name="attend",
    )(
        low, own, high, ctx, mod,
        norm_gain[None, :],
        wq, wk, wv,
        query_gain[None, :],
        key_gain[None, :],
        bias_lines(offset_bias),
    )


def bit_flip(index, bit):
    return index + bit - 2 * bit * ((index // bit) % 2)


def exchange_kernel(
    bits,
    tp_size,
    cond_ref,
    cond_ctx_ref,
    shift_ref,
    scale_ref,
    gate_ref,
    latent_ref,
    context_ref,
    mod_ref,
    low_ref,
    high_ref,
    ctx_ref,
    sums,
    arrived,
    local_sem,
    mod_send,
    mod_recv,
    ctx_send,
    ctx_recv,
    halo_send,
    halo_recv,
    tp_send,
    tp_recv,
):
    me = lax.axis_index("sp")
    mine = lax.axis_index("tp")
    size = lax.axis_size("sp")
    mesh_ids = pl.DeviceIdType.MESH
    barrier = pltpu.get_barrier_semaphore()
    for bit in bits:
        pl.semaphore_signal(
            barrier, inc=1, device_id={"sp": bit_flip(me, bit)}, device_id_type=mesh_ids
        )
    for away in range(1, tp_size):
        pl.semaphore_signal(
            barrier, inc=1, device_id={"tp": (mine + away) % tp_size}, device_id_type=mesh_ids
        )

    for away in (1, size - 1):
        pl.semaphore_signal(
            barrier, inc=1, device_id={"sp": (me + away) % size}, device_id_type=mesh_ids
        )

    share = latent_ref.shape[1] // tp_size
    cols = pl.ds(pl.multiple_of(mine * share, share), share)
    block = context_ref.shape[0]

    def rows_of(mask):
        index = me
        for bit in bits:
            if mask & bit:
                index = bit_flip(index, bit)
        return pl.ds(pl.multiple_of(index * block, block), block)

    keep = pltpu.make_async_copy(
        context_ref.at[:, cols], ctx_ref.at[rows_of(0), cols], local_sem.at[0]
    )
    keep.start()

    def silu(ref):
        v = ref[...].astype(jnp.float32)
        return (v / (1.0 + jnp.exp(-v))).astype(jnp.bfloat16)

    acts = jnp.concatenate([silu(cond_ref), silu(cond_ctx_ref)], axis=0)
    f32 = jnp.float32
    sums[0, 0:2, :] = jnp.dot(acts, shift_ref[...], preferred_element_type=f32)
    sums[0, 2:4, :] = jnp.dot(acts, scale_ref[...], preferred_element_type=f32)
    sums[0, 4:5, :] = jnp.dot(acts, gate_ref[...], preferred_element_type=f32)[0:1]

    pl.semaphore_wait(barrier, len(bits) + tp_size + 1)

    def remote(source, target, send, recv, where):
        return pltpu.make_async_remote_copy(
            src_ref=source, dst_ref=target, send_sem=send, recv_sem=recv,
            device_id=where, device_id_type=mesh_ids,
        )

    tokens = latent_ref.shape[0]
    halo = low_ref.shape[0]
    up = remote(
        latent_ref.at[pl.ds(tokens - halo, halo), cols], low_ref.at[:, cols],
        halo_send.at[0], halo_recv.at[0], {"sp": me + 1},
    )
    down = remote(
        latent_ref.at[pl.ds(0, halo), cols], high_ref.at[:, cols],
        halo_send.at[1], halo_recv.at[1], {"sp": me - 1},
    )
    keep.wait()
    held = [0]
    pending = {}
    started = []
    count = 0
    for step, bit in enumerate(bits):
        where = {"sp": bit_flip(me, bit)}
        term = remote(
            sums.at[step], arrived.at[step], mod_send.at[step], mod_recv.at[step], where
        )
        term.start()
        for mask in list(held):
            if mask in pending:
                pending.pop(mask).wait_recv()
            place = ctx_ref.at[rows_of(mask), cols]
            copy = remote(place, place, ctx_send.at[count], ctx_recv.at[count], where)
            copy.start()
            started.append(copy)
            pending[mask | bit] = remote(
                ctx_ref.at[rows_of(mask | bit), cols], ctx_ref.at[rows_of(mask | bit), cols],
                ctx_send.at[count], ctx_recv.at[count], where,
            )
            held.append(mask | bit)
            count += 1
        if step == 0:

            @pl.when(me < size - 1)
            def _():
                up.start()

            @pl.when(me > 0)
            def _():
                down.start()

        term.wait()
        sums[step + 1] = sums[step] + arrived[step]

    width = sums.shape[2]
    own = pl.ds(pl.multiple_of(mine * width, width), width)
    mod_ref[:, own] = sums[len(bits)]

    def spread(place, slot):
        copies = []
        for away in range(1, tp_size):
            at = slot * (tp_size - 1) + away - 1
            copies.append(
                remote(
                    place, place, tp_send.at[at], tp_recv.at[at], {"tp": (mine + away) % tp_size}
                )
            )
        for copy in copies:
            copy.start()

    def finish(ref, span, slot):
        for away in range(1, tp_size):
            at = slot * (tp_size - 1) + away - 1
            source = (mine + tp_size - away) % tp_size
            came = ref.at[:, pl.ds(pl.multiple_of(source * span, span), span)]
            wait = remote(came, came, tp_send.at[at], tp_recv.at[at], {"tp": source})
            wait.wait_send()
            wait.wait_recv()

    spread(mod_ref.at[:, own], 0)

    @pl.when(me > 0)
    def _():
        up.wait_recv()
        spread(low_ref.at[:, cols], 1)

    @pl.when(me < size - 1)
    def _():
        down.wait_recv()
        spread(high_ref.at[:, cols], 2)

    for mask in list(pending):
        pending.pop(mask).wait_recv()
    spread(ctx_ref.at[:, cols], 3)
    for copy in started:
        copy.wait_send()

    @pl.when(me < size - 1)
    def _():
        up.wait_send()

    @pl.when(me > 0)
    def _():
        down.wait_send()

    finish(mod_ref, width, 0)

    @pl.when(me > 0)
    def _():
        finish(low_ref, share, 1)

    @pl.when(me < size - 1)
    def _():
        finish(high_ref, share, 2)

    finish(ctx_ref, share, 3)


def doubling_order(size):
    bits = [1 << k for k in range(size.bit_length() - 1)]
    return tuple(bits[:1] + bits[:0:-1])


def exchange(latent, context, cond, cond_ctx, shift_weight, scale_weight, gate_weight):
    size, tp_size = lax.axis_size("sp"), lax.axis_size("tp")
    bits = doubling_order(size)
    width = latent.shape[1]
    col_width = shift_weight.shape[1]
    halo = WIN_ROWS // 2 * GRID_W
    vmem = pl.BlockSpec(memory_space=pltpu.VMEM)
    hbm = pl.BlockSpec(memory_space=pl.ANY)
    dma = pltpu.SemaphoreType.DMA
    tp_copies = max(4 * (tp_size - 1), 1)
    f32 = jnp.float32
    return pl.pallas_call(
        functools.partial(exchange_kernel, bits, tp_size),
        out_shape=[
            jax.ShapeDtypeStruct((5, width), f32),
            jax.ShapeDtypeStruct((halo, width), latent.dtype),
            jax.ShapeDtypeStruct((halo, width), latent.dtype),
            jax.ShapeDtypeStruct((context.shape[0] * size, width), context.dtype),
        ],
        in_specs=[vmem] * 5 + [hbm] * 2,
        out_specs=[vmem] * 4,
        scratch_shapes=[
            pltpu.VMEM((len(bits) + 1, 5, col_width), f32),
            pltpu.VMEM((len(bits), 5, col_width), f32),
            dma((1,)),
            dma((len(bits),)),
            dma((len(bits),)),
            dma((size,)),
            dma((size,)),
            dma((2,)),
            dma((2,)),
            dma((tp_copies,)),
            dma((tp_copies,)),
        ],
        compiler_params=pltpu.CompilerParams(collective_id=0, has_side_effects=True),
        name="exchange",
    )(cond[None, :], cond_ctx[None, :], shift_weight, scale_weight, gate_weight, latent, context)


def fast_body(
    latent, context, cond, cond_ctx, shift_weight, scale_weight, gate_weight, norm_gain,
    query_weight, key_weight, value_weight, query_gain, key_gain, offset_bias, out_weight,
):
    col_width = shift_weight.shape[1]
    tp_offset = lax.axis_index("tp") * col_width
    mod, low, high, all_ctx = exchange(
        latent, context, cond, cond_ctx, shift_weight, scale_weight, gate_weight
    )
    total_rows = (latent.shape[0] // GRID_W) * lax.axis_size("sp")
    mixed = attend(
        low, latent, high, all_ctx, mod, norm_gain, query_weight, key_weight, value_weight,
        query_gain, key_gain, offset_bias, total_rows,
    )
    projected = jnp.dot(
        lax.all_gather(mixed, "tp", axis=1, tiled=True),
        out_weight,
        preferred_element_type=jnp.float32,
    )
    own_cols = lax.dynamic_slice_in_dim(latent, tp_offset, col_width, 1).astype(jnp.float32)
    gate_cols = lax.dynamic_slice_in_dim(mod[4], tp_offset, col_width, 0)
    return (own_cols + gate_cols[None, :] * projected).astype(jnp.bfloat16)


LOG2E = 1.4426950408889634


def fused_kernel(
    total_rows,
    latent_ref, context_ref, cond_ref, cond_ctx_ref, shift_ref, scale_ref, gate_ref,
    norm_gain_ref, wq_ref, wk_ref, wv_ref, query_gain_ref, key_gain_ref, table_ref, wo_ref,
    out_ref,
    own_x, low_x, high_x, ctx_x, ws, wq, wk, wv, wo,
    sums, plane_in, sums_z, z_in, final, mod, gain_row,
    q_buf, k_buf, v_buf, ck_buf, cv_buf, lines, bias_buf, bound_buf, ctx_acc, mix,
    local_sem, plane_send, plane_recv, z_send, z_recv, ctx_send, ctx_recv,
    halo_send, halo_recv, tp_send, tp_recv,
):
    f32, bf16 = jnp.float32, jnp.bfloat16
    me, mine = lax.axis_index("sp"), lax.axis_index("tp")
    size = lax.axis_size("sp")
    other = 1 - mine
    mesh_ids = pl.DeviceIdType.MESH
    tokens, width = own_x.shape
    block = context_ref.shape[0]
    share = width // 2
    lane = wq.shape[1]
    pairs = lane // LANES
    rows_dev = tokens // GRID_W
    reach = WIN_ROWS // 2
    halo = reach * GRID_W
    half_ctx = ctx_x.shape[0] // 2
    cols = pl.ds(pl.multiple_of(mine * share, share), share)

    def flip(mask):
        index = me
        bit = 1
        while bit < size:
            if mask & bit:
                index = bit_flip(index, bit)
            bit *= 2
        return index

    def remote(source, target, send, recv, where):
        return pltpu.make_async_remote_copy(
            src_ref=source, dst_ref=target, send_sem=send, recv_sem=recv,
            device_id=where, device_id_type=mesh_ids,
        )

    plane = [1, 2, 3]
    depth = [4 * k for k in sorted(range(1, size // 4), key=lambda k: (k.bit_count(), k))]

    streams = {}
    for place, (name, source, target) in enumerate(
        (
            ("shift", shift_ref, ws.at[0]),
            ("scale", scale_ref, ws.at[1]),
            ("gate", gate_ref, ws.at[2]),
            ("keep", context_ref.at[:, cols],
             ctx_x.at[pl.ds(pl.multiple_of(me * block, block), block), cols]),
            ("own", latent_ref, own_x),
            ("wk", wk_ref, wk),
            ("wv", wv_ref, wv),
            ("wq", wq_ref, wq),
            ("wo", wo_ref, wo),
        )
    ):
        streams[name] = pltpu.make_async_copy(source, target, local_sem.at[place])
        streams[name].start()

    barrier = pltpu.get_barrier_semaphore()
    for mask in plane + depth:
        pl.semaphore_signal(
            barrier, inc=1, device_id={"sp": flip(mask)}, device_id_type=mesh_ids
        )
    pl.semaphore_signal(barrier, inc=1, device_id={"tp": other}, device_id_type=mesh_ids)
    for away in (1, size - 1):
        pl.semaphore_signal(
            barrier, inc=1, device_id={"sp": (me + away) % size}, device_id_type=mesh_ids
        )

    def silu(ref):
        v = ref[...].astype(f32)
        return (v / (1.0 + jnp.exp(-v))).astype(bf16)

    acts = jnp.concatenate([silu(cond_ref), silu(cond_ctx_ref)], axis=0)
    part = share // 2
    for place, name in enumerate(("shift", "scale")):
        streams[name].wait()
        raw = jnp.dot(acts, ws[place], preferred_element_type=f32)
        sums[2 * place : 2 * place + 2, 0:part] = raw[:, :part]
        sums[4 + 2 * place : 6 + 2 * place, 0:part] = raw[:, part:]
    streams["gate"].wait()
    raw = jnp.dot(acts, ws[2], preferred_element_type=f32)
    piece = share // 8
    for k in range(8):
        sums[k : k + 1, part : part + piece] = raw[0:1, k * piece : (k + 1) * piece]

    pl.semaphore_wait(barrier, len(plane) + len(depth) + 3)

    first_stage = []
    for place, mask in enumerate(plane):
        copy = remote(
            sums, plane_in.at[place], plane_send.at[place], plane_recv.at[place],
            {"sp": flip(mask)},
        )
        copy.start()
        first_stage.append(copy)

    slots = {}

    def ctx_copy(mask, toward):
        slot = slots.setdefault((mask, toward), len(slots))
        rows = pl.ds(pl.multiple_of(flip(mask) * block, block), block)
        place = ctx_x.at[rows, cols]
        return remote(
            place, place, ctx_send.at[slot], ctx_recv.at[slot], {"sp": flip(toward)}
        )

    def ctx_arrival(mask, toward):
        slot = slots[(mask, toward)]
        rows = pl.ds(pl.multiple_of(flip(mask ^ toward) * block, block), block)
        place = ctx_x.at[rows, cols]
        remote(place, place, ctx_send.at[slot], ctx_recv.at[slot], {"sp": flip(toward)}).wait_recv()

    streams["keep"].wait()
    started = []

    def ctx_start(mask, toward):
        copy = ctx_copy(mask, toward)
        copy.start()
        started.append(copy)

    ctx_start(0, 1)
    ctx_start(0, 2)

    up = remote(
        latent_ref.at[pl.ds(tokens - halo, halo), cols], low_x.at[:, cols],
        halo_send.at[0], halo_recv.at[0], {"sp": me + 1},
    )
    down = remote(
        latent_ref.at[pl.ds(0, halo), cols], high_x.at[:, cols],
        halo_send.at[1], halo_recv.at[1], {"sp": me - 1},
    )
    even = me % 2 == 0

    @pl.when(even)
    def _():
        up.start()

    @pl.when(jnp.logical_not(even))
    def _():
        down.start()

    @pl.when(jnp.logical_and(even, me > 0))
    def _():
        down.start()

    @pl.when(jnp.logical_and(jnp.logical_not(even), me < size - 1))
    def _():
        up.start()

    for copy in first_stage:
        copy.wait()
    total = sums[...]
    for place in range(len(plane)):
        total = total + plane_in[place]
    sums_z[...] = total
    second_stage = []
    for place, mask in enumerate(depth):
        copy = remote(
            sums_z, z_in.at[place], z_send.at[place], z_recv.at[place], {"sp": flip(mask)}
        )
        copy.start()
        second_stage.append(copy)
    for mask in depth:
        ctx_start(0, mask)
    ctx_arrival(0, 1)
    for mask in depth:
        ctx_start(1, mask)
    ctx_start(1, 2)

    norm_gain = norm_gain_ref[...].astype(f32)
    for k in range(width // LANES):
        gain_row[0:1, k * LANES : (k + 1) * LANES] = norm_gain[k : k + 1, :]
    offsets = table_ref.shape[0]
    span = table_ref.shape[2]
    lines[...] = jnp.zeros_like(lines)
    for k in range(offsets):
        lines[k, :, 0:span] = table_ref[k]
    for k in range(offsets):
        lines[k] = lines[k] + pltpu.roll(lines[k + 1], GRID_W, 1)
    for p in range(pairs):
        filled = jnp.ones((v_buf.shape[0], LANES), bf16)
        v_buf[:, (2 * p + 1) * LANES : (2 * p + 2) * LANES] = filled
        cv_buf[:, (2 * p + 1) * LANES : (2 * p + 2) * LANES] = filled[: cv_buf.shape[0]]

    base = me * rows_dev
    query_col = lax.broadcasted_iota(jnp.int32, (GRID_W, LANES), 0)
    lane_at = lax.broadcasted_iota(jnp.int32, (GRID_W, LANES), 1)
    key_col = lane_at % GRID_W
    window_first = jnp.clip(query_col - WIN_COLS // 2, 0, GRID_W - WIN_COLS)
    inside = (key_col >= window_first) & (key_col < window_first + WIN_COLS)
    per_tile = LANES // GRID_W
    tiles_row = WIN_ROWS // per_tile

    @pl.loop(0, pairs)
    def _(pair):
        for head in range(2):
            for row in range(rows_dev):
                first = jnp.clip(base + row - reach, 0, total_rows - WIN_ROWS)
                offset = first - base - row + WIN_ROWS - 1
                tiles = []
                for tile in range(tiles_row):
                    line = jnp.broadcast_to(
                        lines[offset + tile * per_tile, pl.ds(pair * 2 + head, 1), :],
                        (GRID_W, LANES),
                    )
                    moved = pltpu.roll(line, LANES - (WIN_COLS - 1), 1, stride=1, stride_axis=0)
                    tiles.append(jnp.where(inside, moved, NEG))
                top = tiles[0]
                for tile in tiles[1:]:
                    top = jnp.maximum(top, tile)
                bound = jnp.maximum(jnp.max(top, axis=-1, keepdims=True), 0.0)
                at = pl.ds(head * GRID_W, GRID_W)
                for tile in range(tiles_row):
                    bias_buf[pair, row, at, tile * LANES : (tile + 1) * LANES] = (
                        tiles[tile] - bound
                    ) * LOG2E
                bound_buf[pair, pl.ds(head * tokens + row * GRID_W, GRID_W), :] = jnp.broadcast_to(
                    bound * LOG2E, (GRID_W, LANES)
                )

    for copy in second_stage:
        copy.wait()
    total = sums_z[...]
    for place in range(len(depth)):
        total = total + z_in[place]
    final[0] = total
    swap = remote(final.at[0], final.at[1], tp_send.at[0], tp_recv.at[0], {"tp": other})
    swap.start()
    for mask in depth:
        ctx_arrival(0, mask)
        ctx_arrival(1, mask)
        ctx_start(mask, 2)
        ctx_start(mask ^ 1, 2)
    swap.wait()
    for side in range(2):
        came = final[side]
        at = pl.multiple_of((mine if side == 0 else other) * share, share)
        mod[0:4, pl.ds(at, part)] = came[0:4, 0:part]
        mod[0:4, pl.ds(at + part, part)] = came[4:8, 0:part]
        for k in range(8):
            mod[4:5, pl.ds(at + k * piece, piece)] = came[k : k + 1, part : part + piece]

    norm = gain_row[...]
    wide = 2 * LANES
    half_r = lax.broadcasted_iota(jnp.int32, (wide, wide), 0) // HEAD_DIM
    half_c = lax.broadcasted_iota(jnp.int32, (wide, wide), 1) // HEAD_DIM
    ones = (half_r == half_c).astype(f32).astype(bf16)
    heads = lane // HEAD_DIM
    query_gain = jnp.concatenate(
        [query_gain_ref[...].astype(f32) * (HEAD_DIM ** (-0.5) * LOG2E)] * heads, axis=1
    )
    key_gain = jnp.concatenate([key_gain_ref[...].astype(f32)] * heads, axis=1)

    def normed(raw, gain):
        square = (raw * raw).astype(bf16)
        parts = [
            jnp.dot(square[:, begin : begin + wide], ones, preferred_element_type=f32)
            for begin in range(0, lane, wide)
        ]
        mean = jnp.concatenate(parts, axis=1) * (1.0 / HEAD_DIM)
        return (raw * lax.rsqrt(mean + EPS) * gain).astype(bf16)

    def hidden_of(x, shift, scale):
        values = x.astype(f32)
        inv = lax.rsqrt(jnp.mean(values * values, axis=-1, keepdims=True) + EPS)
        return (values * inv * (norm * (1.0 + scale)) + shift).astype(bf16)

    def keys_values(hidden, k_out, v_out, at):
        count = hidden.shape[0]
        raw = jnp.dot(hidden, wk[...], preferred_element_type=f32)
        k_out[pl.ds(at, count), :] = normed(raw, key_gain)
        raw = jnp.dot(hidden, wv[...], preferred_element_type=f32).astype(bf16)
        for p in range(pairs):
            v_out[pl.ds(at, count), 2 * p * LANES : (2 * p + 1) * LANES] = raw[
                :, p * LANES : (p + 1) * LANES
            ]

    shift, shift_ctx = mod[0:1, :], mod[1:2, :]
    scale, scale_ctx = mod[2:3, :], mod[3:4, :]
    for name in ("own", "wk", "wv", "wq"):
        streams[name].wait()
    hidden = hidden_of(own_x[...], shift, scale)
    keys_values(hidden, k_buf, v_buf, halo)
    q_buf[...] = normed(jnp.dot(hidden, wq[...], preferred_element_type=f32), query_gain)

    def spread(ref, rows, slot):
        copy = remote(
            ref.at[rows, cols], ref.at[rows, cols], tp_send.at[slot], tp_recv.at[slot],
            {"tp": other},
        )
        copy.start()

    def finish(ref, rows, slot):
        theirs = pl.ds(pl.multiple_of(other * share, share), share)
        copy = remote(
            ref.at[rows, theirs], ref.at[rows, theirs], tp_send.at[slot], tp_recv.at[slot],
            {"tp": other},
        )
        copy.wait_send()
        copy.wait_recv()

    every = pl.ds(0, halo)
    for mask in [0, 1] + [m for d in depth for m in (d, d ^ 1)]:
        ctx_arrival(mask, 2)
    all_ctx = pl.ds(0, ctx_x.shape[0])
    spread(ctx_x, all_ctx, 1)

    @pl.when(me > 0)
    def _():
        up.wait_recv()
        spread(low_x, every, 2)

    finish(ctx_x, all_ctx, 1)

    @pl.loop(0, 2)
    def _(part_ctx):
        at = pl.multiple_of(part_ctx * half_ctx, half_ctx)
        hidden = hidden_of(ctx_x[pl.ds(at, half_ctx), :], shift_ctx, scale_ctx)
        keys_values(hidden, ck_buf, cv_buf, at)

    contract = (((1,), (1,)), ((), ()))

    def two_heads(query):
        zero = jnp.zeros_like(query)
        left = lax.broadcasted_iota(jnp.int32, query.shape, 1) < HEAD_DIM
        return jnp.concatenate(
            [jnp.where(left, query, zero), jnp.where(left, zero, query)], axis=0
        )

    @pl.loop(0, pairs)
    def _(pair):
        at = pl.ds(pl.multiple_of(pair * LANES, LANES), LANES)
        at2 = pl.ds(pl.multiple_of(pair * 2 * LANES, 2 * LANES), 2 * LANES)
        score = lax.dot_general(
            two_heads(q_buf[:, at]), ck_buf[:, at], contract, preferred_element_type=f32
        )
        bound = bound_buf[pair]
        shown = jnp.concatenate([bound] * (score.shape[1] // LANES), axis=1)
        weight = jnp.exp2(score - shown).astype(bf16)
        ctx_acc[pair] = jnp.dot(weight, cv_buf[:, at2], preferred_element_type=f32)

    @pl.when(me > 0)
    def _():
        finish(low_x, every, 2)

    keys_values(hidden_of(low_x[...], shift, scale), k_buf, v_buf, 0)

    @pl.when(me < size - 1)
    def _():
        down.wait_recv()
        spread(high_x, every, 3)
        finish(high_x, every, 3)

    keys_values(hidden_of(high_x[...], shift, scale), k_buf, v_buf, halo + tokens)

    def mix_copy(pair):
        at = pl.ds(pl.multiple_of(pair * LANES, LANES), LANES)
        return remote(
            mix.at[0, :, at], mix.at[1, :, at], tp_send.at[4 + pair], tp_recv.at[4 + pair],
            {"tp": other},
        )

    first_head = lane_at < HEAD_DIM

    @pl.loop(0, pairs)
    def _(pair):
        at = pl.ds(pl.multiple_of(pair * LANES, LANES), LANES)
        at2 = pl.ds(pl.multiple_of(pair * 2 * LANES, 2 * LANES), 2 * LANES)
        for row in range(rows_dev):
            first = jnp.clip(base + row - reach, 0, total_rows - WIN_ROWS)
            begin = pl.multiple_of((first - base + reach) * GRID_W, GRID_W)
            mine_rows = slice(row * GRID_W, (row + 1) * GRID_W)
            theirs = slice(tokens + row * GRID_W, tokens + (row + 1) * GRID_W)
            band = pl.ds(begin, WIN_ROWS * GRID_W)
            score = lax.dot_general(
                two_heads(q_buf[mine_rows, at]), k_buf[band, at], contract,
                preferred_element_type=f32,
            )
            weight = jnp.exp2(score + bias_buf[pair, row]).astype(bf16)
            acc = jnp.dot(weight, v_buf[band, at2], preferred_element_type=f32)
            left = acc[:GRID_W] + ctx_acc[pair, mine_rows, :]
            right = acc[GRID_W:] + ctx_acc[pair, theirs, :]
            mix[0, mine_rows, at] = jnp.where(
                first_head,
                left[:, :LANES] / left[:, LANES:],
                right[:, :LANES] / right[:, LANES:],
            ).astype(bf16)
        mix_copy(pair).start()

    streams["wo"].wait()
    out = jnp.dot(
        mix[0], wo[pl.ds(pl.multiple_of(mine * lane, lane), lane), :], preferred_element_type=f32
    )
    for pair in range(pairs):
        mix_copy(pair).wait()
    out = out + jnp.dot(
        mix[1], wo[pl.ds(pl.multiple_of(other * lane, lane), lane), :], preferred_element_type=f32
    )
    out_ref[...] = (own_x[:, cols].astype(f32) + mod[4:5, cols] * out).astype(bf16)

    for copy in started:
        copy.wait_send()

    @pl.when(me < size - 1)
    def _():
        up.wait_send()

    @pl.when(me > 0)
    def _():
        down.wait_send()


def fused_body(
    latent, context, cond, cond_ctx, shift_weight, scale_weight, gate_weight, norm_gain,
    query_weight, key_weight, value_weight, query_gain, key_gain, offset_bias, out_weight,
):
    size = lax.axis_size("sp")
    total_rows = (latent.shape[0] // GRID_W) * size
    tokens, width = latent.shape
    share, lane = shift_weight.shape[1], query_weight.shape[1]
    halo = WIN_ROWS // 2 * GRID_W
    kv_rows = tokens + 2 * halo
    ctx_rows = context.shape[0] * size
    pairs = lane // LANES
    packed = share // 2 + share // 8
    depth = size // 4 - 1
    copies = 4 + 4 * depth
    bf16, f32 = jnp.bfloat16, jnp.float32
    vmem = pl.BlockSpec(memory_space=pltpu.VMEM)
    hbm = pl.BlockSpec(memory_space=pl.ANY)
    dma = pltpu.SemaphoreType.DMA
    return pl.pallas_call(
        functools.partial(fused_kernel, total_rows),
        out_shape=jax.ShapeDtypeStruct((tokens, share), latent.dtype),
        in_specs=[hbm] * 2 + [vmem] * 2 + [hbm] * 3 + [vmem] + [hbm] * 3 + [vmem] * 3 + [hbm],
        out_specs=vmem,
        scratch_shapes=[
            pltpu.VMEM((tokens, width), bf16),
            pltpu.VMEM((halo, width), bf16),
            pltpu.VMEM((halo, width), bf16),
            pltpu.VMEM((ctx_rows, width), bf16),
            pltpu.VMEM((3,) + shift_weight.shape, bf16),
            pltpu.VMEM(query_weight.shape, bf16),
            pltpu.VMEM(key_weight.shape, bf16),
            pltpu.VMEM(value_weight.shape, bf16),
            pltpu.VMEM(out_weight.shape, bf16),
            pltpu.VMEM((8, packed), f32),
            pltpu.VMEM((3, 8, packed), f32),
            pltpu.VMEM((8, packed), f32),
            pltpu.VMEM((depth, 8, packed), f32),
            pltpu.VMEM((2, 8, packed), f32),
            pltpu.VMEM((8, width), f32),
            pltpu.VMEM((1, width), f32),
            pltpu.VMEM((tokens, lane), bf16),
            pltpu.VMEM((kv_rows, lane), bf16),
            pltpu.VMEM((kv_rows, 2 * lane), bf16),
            pltpu.VMEM((ctx_rows, lane), bf16),
            pltpu.VMEM((ctx_rows, 2 * lane), bf16),
            pltpu.VMEM((2 * WIN_ROWS, offset_bias.shape[0], LANES), f32),
            pltpu.VMEM((pairs, tokens // GRID_W, LANES, WIN_ROWS * GRID_W), f32),
            pltpu.VMEM((pairs, 2 * tokens, LANES), f32),
            pltpu.VMEM((pairs, 2 * tokens, 2 * LANES), f32),
            pltpu.VMEM((2, tokens, lane), bf16),
            dma((9,)),
            dma((3,)), dma((3,)),
            dma((depth,)), dma((depth,)),
            dma((copies,)), dma((copies,)),
            dma((2,)), dma((2,)),
            dma((4 + pairs,)), dma((4 + pairs,)),
        ],
        compiler_params=pltpu.CompilerParams(collective_id=0, has_side_effects=True),
        name="fused",
    )(
        latent, context, cond[None, :], cond_ctx[None, :],
        shift_weight, scale_weight, gate_weight,
        norm_gain.reshape(width // LANES, LANES),
        query_weight, key_weight, value_weight,
        query_gain[None, :], key_gain[None, :],
        jnp.transpose(offset_bias, (1, 0, 2)),
        out_weight,
    )


def choose(latent, context, *rest):
    rows_dev = latent.shape[0] // GRID_W
    lane = rest[6].shape[1]
    size = lax.axis_size("sp")
    fits = size >= 4 and size & (size - 1) == 0 and context.shape[0] % 8 == 0
    aligned = lane % LANES == 0 and 2 * GRID_W == LANES
    if fits and aligned and lax.axis_size("tp") == 2 and rows_dev == WIN_ROWS // 2:
        return fused_body(latent, context, *rest)
    if fits and aligned and rows_dev >= WIN_ROWS // 2:
        return fast_body(latent, context, *rest)
    return body(latent, context, *rest)


def solution(mesh):
    in_specs = (
        P("sp", None),
        P("sp", None),
        P("sp"),
        P("sp"),
        P("sp", "tp"),
        P("sp", "tp"),
        P("sp", "tp"),
        P(),
        P(None, "tp"),
        P(None, "tp"),
        P(None, "tp"),
        P(),
        P(),
        P("tp", None, None),
        P(None, "tp"),
    )
    out_specs = P("sp", "tp")
    return jax.shard_map(choose, mesh=mesh, in_specs=in_specs, out_specs=out_specs, check_vma=False)
```

```python
import functools

import jax
import jax.numpy as jnp
import numpy as np
from jax import lax
from jax.experimental import pallas as pl
from jax.experimental.pallas import tpu as pltpu
from jax.sharding import PartitionSpec as P

HEAD_DIM = 64
WIN_ROWS = 8
WIN_COLS = 16
GRID_W = 64


EPS = 1e-06


def padded_2(block, sides, width):
    for axis, dim in sides:
        count = lax.axis_size(axis)
        forward = [(i, i + 1) for i in range(count - 1)]
        backward = [(target, source) for source, target in forward]
        low = lax.ppermute(
            lax.slice_in_dim(block, block.shape[dim] - width, None, axis=dim), axis, forward
        )
        high = lax.ppermute(lax.slice_in_dim(block, 0, width, axis=dim), axis, backward)
        block = jnp.concatenate([low, block, high], axis=dim)
    return block


def modulate(rows, norm_gain, scale, shift):
    values = rows.astype(jnp.float32)
    normed = values * lax.rsqrt(jnp.mean(values * values, axis=-1, keepdims=True) + EPS)
    return (normed * norm_gain.astype(jnp.float32) * (1.0 + scale) + shift).astype(jnp.bfloat16)


def project_heads(hidden, weight, gain):
    raw = jnp.dot(hidden, weight, preferred_element_type=jnp.float32)
    split = raw.reshape(hidden.shape[0], -1, HEAD_DIM)
    if gain is None:
        return split.astype(jnp.bfloat16)
    normed = split * lax.rsqrt(jnp.mean(split * split, axis=-1, keepdims=True) + EPS)
    return (normed * gain.astype(jnp.float32)).astype(jnp.bfloat16)


def body(
    latent,
    context,
    cond,
    cond_ctx,
    shift_weight,
    scale_weight,
    gate_weight,
    norm_gain,
    query_weight,
    key_weight,
    value_weight,
    query_gain,
    key_gain,
    offset_bias,
    out_weight,
):
    width = latent.shape[1]
    col_width = shift_weight.shape[1]
    tp_offset = lax.axis_index("tp") * col_width
    act = jax.nn.silu(cond.astype(jnp.float32)).astype(jnp.bfloat16)
    act_ctx = jax.nn.silu(cond_ctx.astype(jnp.float32)).astype(jnp.bfloat16)
    acts = jnp.stack([act, act_ctx])
    terms = jnp.concatenate(
        [
            jnp.dot(acts, shift_weight, preferred_element_type=jnp.float32),
            jnp.dot(acts, scale_weight, preferred_element_type=jnp.float32),
            jnp.dot(acts[:1], gate_weight, preferred_element_type=jnp.float32),
        ],
        axis=0,
    )
    placed = lax.dynamic_update_slice_in_dim(
        jnp.zeros((5, width), jnp.float32), terms, tp_offset, 1
    )
    full = lax.psum(placed, ("sp", "tp"))
    shift, shift_ctx, scale, scale_ctx, gate = (full[0], full[1], full[2], full[3], full[4])
    heads_dev = offset_bias.shape[0]
    lane = heads_dev * HEAD_DIM
    all_rows = lax.all_gather(context, "sp", axis=0, tiled=True)
    hidden_ctx = modulate(all_rows, norm_gain, scale_ctx, shift_ctx)
    ctx_keys = project_heads(hidden_ctx, key_weight, key_gain)
    ctx_values = project_heads(hidden_ctx, value_weight, None)
    hidden = modulate(latent, norm_gain, scale, shift)
    queries = project_heads(hidden, query_weight, query_gain)
    keys = project_heads(hidden, key_weight, key_gain)
    values = project_heads(hidden, value_weight, None)
    rows_dev = latent.shape[0] // GRID_W
    reach = WIN_ROWS // 2
    grid_kv = jnp.stack(
        [keys.reshape(rows_dev, GRID_W, lane), values.reshape(rows_dev, GRID_W, lane)], axis=1
    )
    padded = padded_2(grid_kv, (("sp", 0),), reach)
    total_rows = rows_dev * lax.axis_size("sp")
    base = lax.axis_index("sp") * rows_dev
    local_rows = base + jnp.arange(rows_dev, dtype=jnp.int32)
    first = jnp.clip(local_rows - reach, 0, total_rows - WIN_ROWS)
    window_rows = jnp.arange(WIN_ROWS, dtype=jnp.int32)
    band_index = (first - base + reach)[:, None] + window_rows[None, :]
    band = jnp.take(padded, band_index, axis=0)
    n_blocks = GRID_W // WIN_COLS
    span = 2 * WIN_COLS
    starts = [
        min(max(block * WIN_COLS - WIN_COLS // 2, 0), GRID_W - span) for block in range(n_blocks)
    ]
    blocked = jnp.stack([band[:, :, :, begin : begin + span] for begin in starts], axis=3)
    blocked = blocked.reshape(rows_dev, WIN_ROWS, 2, n_blocks, span, heads_dev, HEAD_DIM)
    key_blocks = blocked[:, :, 0]
    value_blocks = blocked[:, :, 1]
    query_col = np.arange(n_blocks)[:, None, None] * WIN_COLS + np.arange(WIN_COLS)[None, :, None]
    key_col = np.array(starts)[:, None, None] + np.arange(span)[None, None, :]
    window_first = np.clip(query_col - WIN_COLS // 2, 0, GRID_W - WIN_COLS)
    inside = (key_col >= window_first) & (key_col < window_first + WIN_COLS)
    col_offset = np.clip(key_col - query_col + WIN_COLS - 1, 0, 2 * WIN_COLS - 2)
    col_onehot = (col_offset[..., None] == np.arange(2 * WIN_COLS - 1)).astype(np.float32)
    row_offset = first[:, None] + window_rows[None, :] - local_rows[:, None] + WIN_ROWS - 1
    row_onehot = (row_offset[..., None] == jnp.arange(2 * WIN_ROWS - 1, dtype=jnp.int32)).astype(
        jnp.float32
    )
    by_col = jnp.einsum(
        "hxc,bqkc->hxbqk", offset_bias, jnp.asarray(col_onehot), precision=lax.Precision.HIGHEST
    )
    bias = jnp.einsum("rjx,hxbqk->rhbqjk", row_onehot, by_col, precision=lax.Precision.HIGHEST)
    factor = HEAD_DIM ** (-0.5)
    grid_q = queries.reshape(rows_dev, n_blocks, WIN_COLS, heads_dev, HEAD_DIM)
    local_scores = (
        jnp.einsum("rbqhd,rjbkhd->rhbqjk", grid_q, key_blocks, preferred_element_type=jnp.float32)
        * factor
    )
    local_scores = jnp.where(jnp.asarray(inside)[:, :, None, :], local_scores + bias, -jnp.inf)
    band_len = WIN_ROWS * span
    local_scores = local_scores.reshape(rows_dev, heads_dev, n_blocks, WIN_COLS, band_len)
    ctx_scores = (
        jnp.einsum("rbqhd,chd->rhbqc", grid_q, ctx_keys, preferred_element_type=jnp.float32)
        * factor
    )
    scores = jnp.concatenate([local_scores, ctx_scores], axis=-1)
    top = jnp.max(scores, axis=-1, keepdims=True)
    expd = jnp.exp(scores - top)
    weights = (expd / jnp.sum(expd, axis=-1, keepdims=True)).astype(jnp.bfloat16)
    local_w = weights[..., :band_len].reshape(
        rows_dev, heads_dev, n_blocks, WIN_COLS, WIN_ROWS, span
    )
    mixed = jnp.einsum(
        "rhbqjk,rjbkhd->rbqhd", local_w, value_blocks, preferred_element_type=jnp.float32
    )
    mixed = mixed + jnp.einsum(
        "rhbqc,chd->rbqhd", weights[..., band_len:], ctx_values, preferred_element_type=jnp.float32
    )
    mixed = mixed.astype(jnp.bfloat16).reshape(latent.shape[0], lane)
    projected = jnp.dot(
        lax.all_gather(mixed, "tp", axis=1, tiled=True),
        out_weight,
        preferred_element_type=jnp.float32,
    )
    own_cols = lax.dynamic_slice_in_dim(latent, tp_offset, col_width, 1).astype(jnp.float32)
    gate_cols = lax.dynamic_slice_in_dim(gate, tp_offset, col_width, 0)
    return (own_cols + gate_cols[None, :] * projected).astype(jnp.bfloat16)


LANES = 128
NEG = -1e30


def head_norm(raw, gain, ones):
    square = raw * raw
    high = square.astype(jnp.bfloat16)
    low = (square - high.astype(jnp.float32)).astype(jnp.bfloat16)
    parts = []
    for begin in range(0, raw.shape[1], LANES):
        cut = slice(begin, begin + LANES)
        parts.append(
            jnp.dot(high[:, cut], ones, preferred_element_type=jnp.float32)
            + jnp.dot(low[:, cut], ones, preferred_element_type=jnp.float32)
        )
    mean = jnp.concatenate(parts, axis=1) * (1.0 / HEAD_DIM)
    return raw * lax.rsqrt(mean + EPS) * gain


def attend_kernel(
    total_rows,
    low_ref,
    own_ref,
    high_ref,
    ctx_ref,
    mod_ref,
    norm_gain_ref,
    wq_ref,
    wk_ref,
    wv_ref,
    query_gain_ref,
    key_gain_ref,
    table_ref,
    out_ref,
    q_buf,
    k_buf,
    v_buf,
    ck_buf,
    cv_buf,
    low_vmem,
    own_vmem,
    high_vmem,
    ctx_vmem,
    wq_vmem,
    wk_vmem,
    wv_vmem,
    sems,
):
    tokens, lane = out_ref.shape
    streams = {}
    for place, (name, source, target) in enumerate(
        (
            ("own", own_ref, own_vmem),
            ("wk", wk_ref, wk_vmem),
            ("wv", wv_ref, wv_vmem),
            ("wq", wq_ref, wq_vmem),
            ("low", low_ref, low_vmem),
            ("high", high_ref, high_vmem),
            ("ctx", ctx_ref, ctx_vmem),
        )
    ):
        streams[name] = pltpu.make_async_copy(source, target, sems.at[place])
        streams[name].start()
    rows_dev = tokens // GRID_W
    reach = WIN_ROWS // 2
    halo = reach * GRID_W
    heads = lane // HEAD_DIM
    norm_gain = norm_gain_ref[...].astype(jnp.float32)
    half = lax.broadcasted_iota(jnp.int32, (LANES, LANES), 0) // HEAD_DIM
    half_t = lax.broadcasted_iota(jnp.int32, (LANES, LANES), 1) // HEAD_DIM
    ones = (half == half_t).astype(jnp.float32).astype(jnp.bfloat16)
    query_gain = jnp.concatenate([query_gain_ref[...].astype(jnp.float32)] * heads, axis=1)
    key_gain = jnp.concatenate([key_gain_ref[...].astype(jnp.float32)] * heads, axis=1)

    def hidden_of(x, shift, scale):
        values = x.astype(jnp.float32)
        inv = lax.rsqrt(jnp.mean(values * values, axis=-1, keepdims=True) + EPS)
        return (values * inv * (norm_gain * (1.0 + scale)) + shift).astype(jnp.bfloat16)

    def keys_values(hidden, k_out, v_out, at):
        raw = jnp.dot(hidden, wk_vmem[...], preferred_element_type=jnp.float32)
        k_out[pl.ds(at, hidden.shape[0]), :] = head_norm(raw, key_gain, ones).astype(jnp.bfloat16)
        v_out[pl.ds(at, hidden.shape[0]), :] = jnp.dot(
            hidden, wv_vmem[...], preferred_element_type=jnp.float32
        ).astype(jnp.bfloat16)

    shift, shift_ctx = mod_ref[0:1, :], mod_ref[1:2, :]
    scale, scale_ctx = mod_ref[2:3, :], mod_ref[3:4, :]
    step = min(256, tokens)
    streams["own"].wait()
    for begin in range(0, tokens, step):
        hidden = hidden_of(own_vmem[begin : begin + step, :], shift, scale)
        if begin == 0:
            streams["wk"].wait()
            streams["wv"].wait()
        keys_values(hidden, k_buf, v_buf, halo + begin)
        if begin == 0:
            streams["wq"].wait()
        raw = jnp.dot(hidden, wq_vmem[...], preferred_element_type=jnp.float32)
        q_buf[begin : begin + step, :] = (
            head_norm(raw, query_gain, ones).astype(jnp.bfloat16) * HEAD_DIM ** (-0.5)
        ).astype(jnp.bfloat16)
    streams["low"].wait()
    keys_values(hidden_of(low_vmem[...], shift, scale), k_buf, v_buf, 0)
    streams["high"].wait()
    keys_values(hidden_of(high_vmem[...], shift, scale), k_buf, v_buf, halo + tokens)
    ctx_step = min(256, ctx_vmem.shape[0])
    streams["ctx"].wait()

    @pl.loop(0, ctx_vmem.shape[0] // ctx_step)
    def _(block):
        at = pl.multiple_of(block * ctx_step, ctx_step)
        hidden = hidden_of(ctx_vmem[pl.ds(at, ctx_step), :], shift_ctx, scale_ctx)
        keys_values(hidden, ck_buf, cv_buf, at)

    base = lax.axis_index("sp") * rows_dev
    query_col = lax.broadcasted_iota(jnp.int32, (GRID_W, LANES), 0)
    lane_at = lax.broadcasted_iota(jnp.int32, (GRID_W, LANES), 1)
    key_col = lane_at % GRID_W
    window_first = jnp.clip(query_col - WIN_COLS // 2, 0, GRID_W - WIN_COLS)
    inside = (key_col >= window_first) & (key_col < window_first + WIN_COLS)
    first_head = lane_at < HEAD_DIM
    per_tile = LANES // GRID_W
    contract = (((1,), (1,)), ((), ()))

    @pl.loop(0, lane // LANES)
    def _(pair):
        cols = pl.ds(pl.multiple_of(pair * LANES, LANES), LANES)
        for row in range(rows_dev):
            first = jnp.clip(base + row - reach, 0, total_rows - WIN_ROWS)
            begin = pl.multiple_of((first - base + reach) * GRID_W, GRID_W)
            offset = first - base - row + WIN_ROWS - 1
            mine = slice(row * GRID_W, (row + 1) * GRID_W)
            query = q_buf[mine, cols]
            zero = jnp.zeros_like(query)
            query2 = jnp.concatenate(
                [jnp.where(first_head, query, zero), jnp.where(first_head, zero, query)], axis=0
            )
            band = pl.ds(begin, WIN_ROWS * GRID_W)
            local = lax.dot_general(
                query2, k_buf[band, cols], contract, preferred_element_type=jnp.float32
            )
            ctx = lax.dot_general(
                query2, ck_buf[:, cols], contract, preferred_element_type=jnp.float32
            )
            biases = []
            for head in range(2):
                tiles = []
                for tile in range(WIN_ROWS // per_tile):
                    entry = (pair * 2 + head) * (2 * WIN_ROWS) + offset + tile * per_tile
                    line = jnp.broadcast_to(table_ref[entry], (GRID_W, LANES))
                    moved = pltpu.roll(line, LANES - (WIN_COLS - 1), 1, stride=1, stride_axis=0)
                    tiles.append(jnp.where(inside, moved, NEG))
                biases.append(jnp.concatenate(tiles, axis=1))
            local = local + jnp.concatenate(biases, axis=0)
            top = jnp.maximum(
                jnp.max(local, axis=-1, keepdims=True), jnp.max(ctx, axis=-1, keepdims=True)
            )
            local = jnp.exp(local - top)
            ctx = jnp.exp(ctx - top)
            total = jnp.sum(local, axis=-1, keepdims=True) + jnp.sum(ctx, axis=-1, keepdims=True)
            mixed = jnp.dot(
                local.astype(jnp.bfloat16), v_buf[band, cols], preferred_element_type=jnp.float32
            ) + jnp.dot(
                ctx.astype(jnp.bfloat16), cv_buf[:, cols], preferred_element_type=jnp.float32
            )
            mixed = mixed / total
            out_ref[mine, cols] = jnp.where(
                first_head, mixed[:GRID_W], mixed[GRID_W:]
            ).astype(jnp.bfloat16)


def bias_lines(offset_bias):
    heads = offset_bias.shape[0]
    wide = jnp.pad(offset_bias, ((0, 0), (0, 2), (0, GRID_W - offset_bias.shape[2])))
    lines = jnp.concatenate([wide[:, :-1], wide[:, 1:]], axis=2)
    return lines.reshape(heads * 2 * WIN_ROWS, 1, LANES)


def attend(
    low, own, high, ctx, mod, norm_gain, wq, wk, wv, query_gain, key_gain, offset_bias, total_rows
):
    tokens, lane = own.shape[0], wq.shape[1]
    halo = low.shape[0]
    rows = tokens + 2 * halo
    vmem = pl.BlockSpec(memory_space=pltpu.VMEM)
    hbm = pl.BlockSpec(memory_space=pl.ANY)
    return pl.pallas_call(
        functools.partial(attend_kernel, total_rows),
        out_shape=jax.ShapeDtypeStruct((tokens, lane), jnp.bfloat16),
        in_specs=[hbm] * 4 + [vmem] * 2 + [hbm] * 3 + [vmem] * 3,
        out_specs=vmem,
        scratch_shapes=[
            pltpu.VMEM((tokens, lane), jnp.bfloat16),
            pltpu.VMEM((rows, lane), jnp.bfloat16),
            pltpu.VMEM((rows, lane), jnp.bfloat16),
            pltpu.VMEM((ctx.shape[0], lane), jnp.bfloat16),
            pltpu.VMEM((ctx.shape[0], lane), jnp.bfloat16),
        ]
        + [pltpu.VMEM(x.shape, x.dtype) for x in (low, own, high, ctx, wq, wk, wv)]
        + [pltpu.SemaphoreType.DMA((7,))],
        cost_estimate=pl.CostEstimate(
            flops=12 * tokens * own.shape[1] * lane, bytes_accessed=1 << 24, transcendentals=1 << 21
        ),
        name="attend",
    )(
        low, own, high, ctx, mod,
        norm_gain[None, :],
        wq, wk, wv,
        query_gain[None, :],
        key_gain[None, :],
        bias_lines(offset_bias),
    )


def bit_flip(index, bit):
    return index + bit - 2 * bit * ((index // bit) % 2)


def exchange_kernel(
    bits,
    tp_size,
    cond_ref,
    cond_ctx_ref,
    shift_ref,
    scale_ref,
    gate_ref,
    latent_ref,
    context_ref,
    mod_ref,
    low_ref,
    high_ref,
    ctx_ref,
    sums,
    arrived,
    local_sem,
    mod_send,
    mod_recv,
    ctx_send,
    ctx_recv,
    halo_send,
    halo_recv,
    tp_send,
    tp_recv,
):
    me = lax.axis_index("sp")
    mine = lax.axis_index("tp")
    size = lax.axis_size("sp")
    mesh_ids = pl.DeviceIdType.MESH
    barrier = pltpu.get_barrier_semaphore()
    for bit in bits:
        pl.semaphore_signal(
            barrier, inc=1, device_id={"sp": bit_flip(me, bit)}, device_id_type=mesh_ids
        )
    for away in range(1, tp_size):
        pl.semaphore_signal(
            barrier, inc=1, device_id={"tp": (mine + away) % tp_size}, device_id_type=mesh_ids
        )

    for away in (1, size - 1):
        pl.semaphore_signal(
            barrier, inc=1, device_id={"sp": (me + away) % size}, device_id_type=mesh_ids
        )

    share = latent_ref.shape[1] // tp_size
    cols = pl.ds(pl.multiple_of(mine * share, share), share)
    block = context_ref.shape[0]

    def rows_of(mask):
        index = me
        for bit in bits:
            if mask & bit:
                index = bit_flip(index, bit)
        return pl.ds(pl.multiple_of(index * block, block), block)

    keep = pltpu.make_async_copy(
        context_ref.at[:, cols], ctx_ref.at[rows_of(0), cols], local_sem.at[0]
    )
    keep.start()

    def silu(ref):
        v = ref[...].astype(jnp.float32)
        return (v / (1.0 + jnp.exp(-v))).astype(jnp.bfloat16)

    acts = jnp.concatenate([silu(cond_ref), silu(cond_ctx_ref)], axis=0)
    f32 = jnp.float32
    sums[0, 0:2, :] = jnp.dot(acts, shift_ref[...], preferred_element_type=f32)
    sums[0, 2:4, :] = jnp.dot(acts, scale_ref[...], preferred_element_type=f32)
    sums[0, 4:5, :] = jnp.dot(acts, gate_ref[...], preferred_element_type=f32)[0:1]

    pl.semaphore_wait(barrier, len(bits) + tp_size + 1)

    def remote(source, target, send, recv, where):
        return pltpu.make_async_remote_copy(
            src_ref=source, dst_ref=target, send_sem=send, recv_sem=recv,
            device_id=where, device_id_type=mesh_ids,
        )

    tokens = latent_ref.shape[0]
    halo = low_ref.shape[0]
    up = remote(
        latent_ref.at[pl.ds(tokens - halo, halo), cols], low_ref.at[:, cols],
        halo_send.at[0], halo_recv.at[0], {"sp": me + 1},
    )
    down = remote(
        latent_ref.at[pl.ds(0, halo), cols], high_ref.at[:, cols],
        halo_send.at[1], halo_recv.at[1], {"sp": me - 1},
    )
    keep.wait()
    held = [0]
    pending = {}
    started = []
    count = 0
    for step, bit in enumerate(bits):
        where = {"sp": bit_flip(me, bit)}
        term = remote(
            sums.at[step], arrived.at[step], mod_send.at[step], mod_recv.at[step], where
        )
        term.start()
        for mask in list(held):
            if mask in pending:
                pending.pop(mask).wait_recv()
            place = ctx_ref.at[rows_of(mask), cols]
            copy = remote(place, place, ctx_send.at[count], ctx_recv.at[count], where)
            copy.start()
            started.append(copy)
            pending[mask | bit] = remote(
                ctx_ref.at[rows_of(mask | bit), cols], ctx_ref.at[rows_of(mask | bit), cols],
                ctx_send.at[count], ctx_recv.at[count], where,
            )
            held.append(mask | bit)
            count += 1
        if step == 0:

            @pl.when(me < size - 1)
            def _():
                up.start()

            @pl.when(me > 0)
            def _():
                down.start()

        term.wait()
        sums[step + 1] = sums[step] + arrived[step]

    width = sums.shape[2]
    own = pl.ds(pl.multiple_of(mine * width, width), width)
    mod_ref[:, own] = sums[len(bits)]

    def spread(place, slot):
        copies = []
        for away in range(1, tp_size):
            at = slot * (tp_size - 1) + away - 1
            copies.append(
                remote(
                    place, place, tp_send.at[at], tp_recv.at[at], {"tp": (mine + away) % tp_size}
                )
            )
        for copy in copies:
            copy.start()

    def finish(ref, span, slot):
        for away in range(1, tp_size):
            at = slot * (tp_size - 1) + away - 1
            source = (mine + tp_size - away) % tp_size
            came = ref.at[:, pl.ds(pl.multiple_of(source * span, span), span)]
            wait = remote(came, came, tp_send.at[at], tp_recv.at[at], {"tp": source})
            wait.wait_send()
            wait.wait_recv()

    spread(mod_ref.at[:, own], 0)

    @pl.when(me > 0)
    def _():
        up.wait_recv()
        spread(low_ref.at[:, cols], 1)

    @pl.when(me < size - 1)
    def _():
        down.wait_recv()
        spread(high_ref.at[:, cols], 2)

    for mask in list(pending):
        pending.pop(mask).wait_recv()
    spread(ctx_ref.at[:, cols], 3)
    for copy in started:
        copy.wait_send()

    @pl.when(me < size - 1)
    def _():
        up.wait_send()

    @pl.when(me > 0)
    def _():
        down.wait_send()

    finish(mod_ref, width, 0)

    @pl.when(me > 0)
    def _():
        finish(low_ref, share, 1)

    @pl.when(me < size - 1)
    def _():
        finish(high_ref, share, 2)

    finish(ctx_ref, share, 3)


def doubling_order(size):
    bits = [1 << k for k in range(size.bit_length() - 1)]
    return tuple(bits[:1] + bits[:0:-1])


def exchange(latent, context, cond, cond_ctx, shift_weight, scale_weight, gate_weight):
    size, tp_size = lax.axis_size("sp"), lax.axis_size("tp")
    bits = doubling_order(size)
    width = latent.shape[1]
    col_width = shift_weight.shape[1]
    halo = WIN_ROWS // 2 * GRID_W
    vmem = pl.BlockSpec(memory_space=pltpu.VMEM)
    hbm = pl.BlockSpec(memory_space=pl.ANY)
    dma = pltpu.SemaphoreType.DMA
    tp_copies = max(4 * (tp_size - 1), 1)
    f32 = jnp.float32
    return pl.pallas_call(
        functools.partial(exchange_kernel, bits, tp_size),
        out_shape=[
            jax.ShapeDtypeStruct((5, width), f32),
            jax.ShapeDtypeStruct((halo, width), latent.dtype),
            jax.ShapeDtypeStruct((halo, width), latent.dtype),
            jax.ShapeDtypeStruct((context.shape[0] * size, width), context.dtype),
        ],
        in_specs=[vmem] * 5 + [hbm] * 2,
        out_specs=[vmem] * 4,
        scratch_shapes=[
            pltpu.VMEM((len(bits) + 1, 5, col_width), f32),
            pltpu.VMEM((len(bits), 5, col_width), f32),
            dma((1,)),
            dma((len(bits),)),
            dma((len(bits),)),
            dma((size,)),
            dma((size,)),
            dma((2,)),
            dma((2,)),
            dma((tp_copies,)),
            dma((tp_copies,)),
        ],
        compiler_params=pltpu.CompilerParams(collective_id=0, has_side_effects=True),
        name="exchange",
    )(cond[None, :], cond_ctx[None, :], shift_weight, scale_weight, gate_weight, latent, context)


def fast_body(
    latent, context, cond, cond_ctx, shift_weight, scale_weight, gate_weight, norm_gain,
    query_weight, key_weight, value_weight, query_gain, key_gain, offset_bias, out_weight,
):
    col_width = shift_weight.shape[1]
    tp_offset = lax.axis_index("tp") * col_width
    mod, low, high, all_ctx = exchange(
        latent, context, cond, cond_ctx, shift_weight, scale_weight, gate_weight
    )
    total_rows = (latent.shape[0] // GRID_W) * lax.axis_size("sp")
    mixed = attend(
        low, latent, high, all_ctx, mod, norm_gain, query_weight, key_weight, value_weight,
        query_gain, key_gain, offset_bias, total_rows,
    )
    projected = jnp.dot(
        lax.all_gather(mixed, "tp", axis=1, tiled=True),
        out_weight,
        preferred_element_type=jnp.float32,
    )
    own_cols = lax.dynamic_slice_in_dim(latent, tp_offset, col_width, 1).astype(jnp.float32)
    gate_cols = lax.dynamic_slice_in_dim(mod[4], tp_offset, col_width, 0)
    return (own_cols + gate_cols[None, :] * projected).astype(jnp.bfloat16)


LOG2E = 1.4426950408889634


def fused_kernel(
    total_rows,
    latent_ref, context_ref, cond_hbm, cond_ctx_hbm, shift_ref, scale_ref, gate_ref,
    norm_gain_hbm, wq_ref, wk_ref, wv_ref, query_gain_hbm, key_gain_hbm, table_hbm, wo_ref,
    out_ref,
    cond_ref, cond_ctx_ref, norm_gain_ref, query_gain_ref, key_gain_ref, table_ref,
    own_x, halo_x, ctx_x, ws, wq, wk, wv, wo,
    sums, plane_in, sums_z, z_in, final, mod, gain_row,
    q_buf, k_buf, v_buf, ck_buf, cv_buf, lines, bias_buf, bound_buf, near, mix,
    local_sem, plane_send, plane_recv, z_send, z_recv, ctx_send, ctx_recv,
    halo_send, halo_recv, relay_send, relay_recv, tp_send, tp_recv,
):
    f32, bf16 = jnp.float32, jnp.bfloat16
    me, mine = lax.axis_index("sp"), lax.axis_index("tp")
    size = lax.axis_size("sp")
    other = 1 - mine
    mesh_ids = pl.DeviceIdType.MESH
    tokens, width = own_x.shape
    block = context_ref.shape[0]
    share = width // 2
    lane = wq.shape[1]
    pairs = lane // LANES
    rows_dev = tokens // GRID_W
    reach = WIN_ROWS // 2
    halo = reach * GRID_W
    half_ctx = ctx_x.shape[0] // 2
    cols = pl.ds(pl.multiple_of(mine * share, share), share)

    def flip(mask):
        index = me
        bit = 1
        while bit < size:
            if mask & bit:
                index = bit_flip(index, bit)
            bit *= 2
        return index

    def remote(source, target, send, recv, where):
        return pltpu.make_async_remote_copy(
            src_ref=source, dst_ref=target, send_sem=send, recv_sem=recv,
            device_id=where, device_id_type=mesh_ids,
        )

    plane = [1, 2, 3]
    depth = [4 * k for k in sorted(range(1, size // 4), key=lambda k: (k.bit_count(), k))]

    streams = {}
    for place, (name, source, target) in enumerate(
        (
            ("cond", cond_hbm, cond_ref),
            ("cond_ctx", cond_ctx_hbm, cond_ctx_ref),
            ("shift", shift_ref, ws.at[0]),
            ("scale", scale_ref, ws.at[1]),
            ("gate", gate_ref, ws.at[2]),
            ("keep", context_ref.at[:, cols],
             ctx_x.at[pl.ds(pl.multiple_of(me * block, block), block), cols]),
            ("table", table_hbm, table_ref),
            ("norm_gain", norm_gain_hbm, norm_gain_ref),
            ("query_gain", query_gain_hbm, query_gain_ref),
            ("key_gain", key_gain_hbm, key_gain_ref),
            ("own", latent_ref, own_x),
            ("wk", wk_ref, wk),
            ("wv", wv_ref, wv),
            ("wq", wq_ref, wq),
            ("wo", wo_ref, wo),
        )
    ):
        streams[name] = pltpu.make_async_copy(source, target, local_sem.at[place])

    def fetch(*names):
        for name in names:
            streams[name].start()

    def arrived(*names):
        for name in names:
            streams[name].wait()

    fetch("cond", "cond_ctx", "shift", "scale", "gate", "keep", "table")
    fetch("norm_gain", "query_gain", "key_gain")

    barrier = pltpu.get_barrier_semaphore()
    for mask in plane + depth:
        pl.semaphore_signal(
            barrier, inc=1, device_id={"sp": flip(mask)}, device_id_type=mesh_ids
        )
    pl.semaphore_signal(barrier, inc=1, device_id={"tp": other}, device_id_type=mesh_ids)
    parity = me % 2
    ahead = me + 2 - 4 * parity
    behind = me - 2 + 4 * parity
    pl.semaphore_signal(
        barrier, inc=1, device_id={"sp": (ahead + size) % size}, device_id_type=mesh_ids
    )
    pl.semaphore_signal(
        barrier, inc=1, device_id={"sp": (behind + size) % size}, device_id_type=mesh_ids
    )

    def silu(ref):
        v = ref[...].astype(f32)
        return (v / (1.0 + jnp.exp(-v))).astype(bf16)

    arrived("cond", "cond_ctx", "shift", "scale", "gate")
    fetch("own", "wk", "wv", "wq", "wo")
    acts = jnp.concatenate([silu(cond_ref), silu(cond_ctx_ref)], axis=0)
    part = share // 2
    for place in range(2):
        raw = jnp.dot(acts, ws[place], preferred_element_type=f32)
        sums[2 * place : 2 * place + 2, 0:part] = raw[:, :part]
        sums[4 + 2 * place : 6 + 2 * place, 0:part] = raw[:, part:]
    raw = jnp.dot(acts, ws[2], preferred_element_type=f32)
    piece = share // 8
    for k in range(8):
        sums[k : k + 1, part : part + piece] = raw[0:1, k * piece : (k + 1) * piece]

    arrived("keep", "table", "norm_gain", "query_gain", "key_gain")
    norm_gain = norm_gain_ref[...].astype(f32)
    for k in range(width // LANES):
        gain_row[0:1, k * LANES : (k + 1) * LANES] = norm_gain[k : k + 1, :]
    offsets = table_ref.shape[0]
    span = table_ref.shape[2]
    lines[...] = jnp.zeros_like(lines)
    for k in range(offsets):
        lines[k, :, 0:span] = table_ref[k]
    for k in range(offsets):
        lines[k] = lines[k] + pltpu.roll(lines[k + 1], GRID_W, 1)
    for p in range(pairs):
        filled = jnp.ones((v_buf.shape[0], LANES), bf16)
        v_buf[:, (2 * p + 1) * LANES : (2 * p + 2) * LANES] = filled
        cv_buf[:, (2 * p + 1) * LANES : (2 * p + 2) * LANES] = filled[: cv_buf.shape[0]]

    base = me * rows_dev
    query_col = lax.broadcasted_iota(jnp.int32, (GRID_W, LANES), 0)
    lane_at = lax.broadcasted_iota(jnp.int32, (GRID_W, LANES), 1)
    key_col = lane_at % GRID_W
    window_first = jnp.clip(query_col - WIN_COLS // 2, 0, GRID_W - WIN_COLS)
    inside = (key_col >= window_first) & (key_col < window_first + WIN_COLS)
    per_tile = LANES // GRID_W
    tiles_row = WIN_ROWS // per_tile

    def bias_of(pair):
        for head in range(2):
            for row in range(rows_dev):
                first = jnp.clip(base + row - reach, 0, total_rows - WIN_ROWS)
                offset = first - base - row + WIN_ROWS - 1
                tiles = []
                for tile in range(tiles_row):
                    line = jnp.broadcast_to(
                        lines[offset + tile * per_tile, pl.ds(pair * 2 + head, 1), :],
                        (GRID_W, LANES),
                    )
                    moved = pltpu.roll(line, LANES - (WIN_COLS - 1), 1, stride=1, stride_axis=0)
                    tiles.append(jnp.where(inside, moved, NEG))
                top = tiles[0]
                for tile in tiles[1:]:
                    top = jnp.maximum(top, tile)
                bound = jnp.maximum(jnp.max(top, axis=-1, keepdims=True), 0.0)
                at = pl.ds(head * GRID_W, GRID_W)
                for tile in range(tiles_row):
                    bias_buf[pair, row, at, tile * LANES : (tile + 1) * LANES] = (
                        tiles[tile] - bound
                    ) * LOG2E
                bound_buf[pair, pl.ds(head * tokens + row * GRID_W, GRID_W), :] = jnp.broadcast_to(
                    bound * LOG2E, (GRID_W, LANES)
                )

    quarter = pairs // 4
    pl.loop(0, quarter)(bias_of)
    pl.semaphore_wait(barrier, len(plane) + len(depth) + 3)

    first_stage = []
    for place, mask in enumerate(plane):
        copy = remote(
            sums, plane_in.at[place], plane_send.at[place], plane_recv.at[place],
            {"sp": flip(mask)},
        )
        copy.start()
        first_stage.append(copy)

    slots = {}

    def ctx_copy(mask, toward):
        slot = slots.setdefault((mask, toward), len(slots))
        rows = pl.ds(pl.multiple_of(flip(mask) * block, block), block)
        place = ctx_x.at[rows, cols]
        return remote(
            place, place, ctx_send.at[slot], ctx_recv.at[slot], {"sp": flip(toward)}
        )

    def ctx_arrival(mask, toward):
        slot = slots[(mask, toward)]
        rows = pl.ds(pl.multiple_of(flip(mask ^ toward) * block, block), block)
        place = ctx_x.at[rows, cols]
        remote(place, place, ctx_send.at[slot], ctx_recv.at[slot], {"sp": flip(toward)}).wait_recv()

    started = []

    def ctx_start(mask, toward):
        copy = ctx_copy(mask, toward)
        copy.start()
        started.append(copy)

    ctx_start(0, 1)
    ctx_start(0, 2)

    chunks = reach
    step = halo // chunks

    def partner_copy(k):
        rows = pl.ds(k * step, step)
        return remote(
            latent_ref.at[rows, cols], halo_x.at[parity, rows, cols],
            halo_send.at[k], halo_recv.at[k], {"sp": flip(1)},
        )

    def relay_copy(k):
        rows = pl.ds(k * step, step)
        return remote(
            halo_x.at[1 - parity, rows, cols], halo_x.at[parity, rows, cols],
            relay_send.at[k], relay_recv.at[k], {"sp": ahead},
        )

    has_ahead = jnp.logical_and(ahead >= 0, ahead < size)
    has_behind = jnp.logical_and(behind >= 0, behind < size)

    def spread(ref, rows, slot):
        remote(
            ref.at[rows, cols], ref.at[rows, cols], tp_send.at[slot], tp_recv.at[slot],
            {"tp": other},
        ).start()

    def finish(ref, rows, slot):
        theirs = pl.ds(pl.multiple_of(other * share, share), share)
        copy = remote(
            ref.at[rows, theirs], ref.at[rows, theirs], tp_send.at[slot], tp_recv.at[slot],
            {"tp": other},
        )
        copy.wait_send()
        copy.wait_recv()

    def relay(k):
        partner_copy(k).wait_recv()

        @pl.when(has_ahead)
        def _():
            relay_copy(k).start()

        spread(halo_x.at[1 - parity], pl.ds(k * step, step), 1 + k)

    def plane_rows(mask):
        return pl.ds(pl.multiple_of(flip(mask) // 4 * 4 * block, 4 * block), 4 * block)

    def plane_slot(mask):
        return 1 + 2 * chunks + mask // 4

    near_masks = [mask for mask in depth if mask < size // 2]
    far_masks = [mask for mask in depth if mask >= size // 2][::-1]
    via_x, via_y = far_masks[: len(far_masks) // 2], far_masks[len(far_masks) // 2 :]
    partner_copy(0).start()
    for mask in near_masks:
        ctx_start(0, mask)

    pl.loop(quarter, 2 * quarter)(bias_of)
    for copy in first_stage:
        copy.wait()
    total = sums[...]
    for place in range(len(plane)):
        total = total + plane_in[place]
    sums_z[...] = total
    second_stage = []
    for place, mask in enumerate(depth):
        copy = remote(
            sums_z, z_in.at[place], z_send.at[place], z_recv.at[place], {"sp": flip(mask)}
        )
        copy.start()
        second_stage.append(copy)
    ctx_arrival(0, 1)
    ctx_start(1, 2)
    for mask in near_masks:
        ctx_arrival(0, mask)
        ctx_start(mask, 1)
        ctx_start(mask, 2)
    for k in range(1, chunks):
        partner_copy(k).start()

    pl.loop(2 * quarter, 3 * quarter)(bias_of)
    relay(0)
    pl.loop(3 * quarter, pairs)(bias_of)
    for copy in second_stage:
        copy.wait()
    total = sums_z[...]
    for place in range(len(depth)):
        total = total + z_in[place]
    final[0] = total
    swap = remote(final.at[0], final.at[1], tp_send.at[0], tp_recv.at[0], {"tp": other})
    swap.start()
    for mask in far_masks:
        ctx_start(0, mask)
    ctx_arrival(0, 2)
    ctx_arrival(1, 2)
    spread(ctx_x, plane_rows(0), plane_slot(0))
    for mask in near_masks:
        ctx_arrival(mask, 1)
        ctx_start(mask ^ 1, 2)
    swap.wait()
    for side in range(2):
        came = final[side]
        at = pl.multiple_of((mine if side == 0 else other) * share, share)
        mod[0:4, pl.ds(at, part)] = came[0:4, 0:part]
        mod[0:4, pl.ds(at + part, part)] = came[4:8, 0:part]
        for k in range(8):
            mod[4:5, pl.ds(at + k * piece, piece)] = came[k : k + 1, part : part + piece]

    norm = gain_row[...]
    wide = 2 * LANES
    half_r = lax.broadcasted_iota(jnp.int32, (wide, wide), 0) // HEAD_DIM
    half_c = lax.broadcasted_iota(jnp.int32, (wide, wide), 1) // HEAD_DIM
    ones = (half_r == half_c).astype(f32).astype(bf16)
    heads = lane // HEAD_DIM
    query_gain = jnp.concatenate(
        [query_gain_ref[...].astype(f32) * (HEAD_DIM ** (-0.5) * LOG2E)] * heads, axis=1
    )
    key_gain = jnp.concatenate([key_gain_ref[...].astype(f32)] * heads, axis=1)

    def normed(raw, gain):
        square = (raw * raw).astype(bf16)
        parts = [
            jnp.dot(square[:, begin : begin + wide], ones, preferred_element_type=f32)
            for begin in range(0, lane, wide)
        ]
        mean = jnp.concatenate(parts, axis=1) * (1.0 / HEAD_DIM)
        return (raw * lax.rsqrt(mean + EPS) * gain).astype(bf16)

    def hidden_of(x, shift, scale):
        values = x.astype(f32)
        inv = lax.rsqrt(jnp.mean(values * values, axis=-1, keepdims=True) + EPS)
        return (values * inv * (norm * (1.0 + scale)) + shift).astype(bf16)

    def keys_values(hidden, k_out, v_out, at):
        count = hidden.shape[0]
        raw = jnp.dot(hidden, wk[...], preferred_element_type=f32)
        k_out[pl.ds(at, count), :] = normed(raw, key_gain)
        raw = jnp.dot(hidden, wv[...], preferred_element_type=f32).astype(bf16)
        for p in range(pairs):
            v_out[pl.ds(at, count), 2 * p * LANES : (2 * p + 1) * LANES] = raw[
                :, p * LANES : (p + 1) * LANES
            ]

    shift, shift_ctx = mod[0:1, :], mod[1:2, :]
    scale, scale_ctx = mod[2:3, :], mod[3:4, :]
    arrived("own", "wk", "wv", "wq")
    hidden = hidden_of(own_x[...], shift, scale)
    keys_values(hidden, k_buf, v_buf, halo)
    relay(1)
    q_buf[...] = normed(jnp.dot(hidden, wq[...], preferred_element_type=f32), query_gain)

    for mask in near_masks:
        ctx_arrival(mask, 2)
        ctx_arrival(mask ^ 1, 2)
        spread(ctx_x, plane_rows(mask), plane_slot(mask))
    for mask in [0] + near_masks:
        finish(ctx_x, plane_rows(mask), plane_slot(mask))

    def between(far):
        if far:
            return
        relay(2)
        for mask in far_masks:
            ctx_arrival(0, mask)
            ctx_start(mask, 1)

    def ctx_half(far):
        top = size // 2
        index = me // top
        if far:
            index = 1 - index
        at = pl.multiple_of(index * half_ctx, half_ctx)
        hidden = hidden_of(ctx_x[pl.ds(at, half_ctx), :], shift_ctx, scale_ctx)
        between(far)
        keys_values(hidden, ck_buf, cv_buf, at)
        return pl.ds(at, half_ctx)

    near_rows = ctx_half(False)

    contract = (((1,), (1,)), ((), ()))

    def two_heads(query):
        zero = jnp.zeros_like(query)
        left = lax.broadcasted_iota(jnp.int32, query.shape, 1) < HEAD_DIM
        return jnp.concatenate(
            [jnp.where(left, query, zero), jnp.where(left, zero, query)], axis=0
        )

    def from_ctx(pair, rows):
        at = pl.ds(pl.multiple_of(pair * LANES, LANES), LANES)
        at2 = pl.ds(pl.multiple_of(pair * 2 * LANES, 2 * LANES), 2 * LANES)
        score = lax.dot_general(
            two_heads(q_buf[:, at]), ck_buf[rows, at], contract, preferred_element_type=f32
        )
        shown = jnp.concatenate([bound_buf[pair]] * (half_ctx // LANES), axis=1)
        weight = jnp.exp2(score - shown).astype(bf16)
        return jnp.dot(weight, cv_buf[rows, at2], preferred_element_type=f32)

    @pl.loop(0, pairs)
    def _(pair):
        near[pair] = from_ctx(pair, near_rows)

    for k in range(3, chunks):
        relay(k)
    for mask in far_masks:
        ctx_start(mask, 2)
    for k in range(chunks):
        finish(halo_x.at[1 - parity], pl.ds(k * step, step), 1 + k)
    stride = halo + tokens
    keys_values(
        hidden_of(halo_x[1 - parity], shift, scale),
        k_buf, v_buf, pl.multiple_of((1 - parity) * stride, stride),
    )
    for mask in via_y:
        ctx_arrival(mask, 1)
        ctx_start(mask ^ 1, 2)

    @pl.when(has_behind)
    def _():
        for k in range(chunks):
            relay_copy(k).wait_recv()
            spread(halo_x.at[parity], pl.ds(k * step, step), 1 + chunks + k)

    for mask in via_x:
        ctx_arrival(mask, 2)
        ctx_start(mask ^ 2, 1)

    @pl.when(has_behind)
    def _():
        for k in range(chunks):
            finish(halo_x.at[parity], pl.ds(k * step, step), 1 + chunks + k)

    keys_values(
        hidden_of(halo_x[parity], shift, scale),
        k_buf, v_buf, pl.multiple_of(parity * stride, stride),
    )

    def from_window(pair):
        at = pl.ds(pl.multiple_of(pair * LANES, LANES), LANES)
        at2 = pl.ds(pl.multiple_of(pair * 2 * LANES, 2 * LANES), 2 * LANES)
        for row in range(rows_dev):
            first = jnp.clip(base + row - reach, 0, total_rows - WIN_ROWS)
            begin = pl.multiple_of((first - base + reach) * GRID_W, GRID_W)
            mine_rows = slice(row * GRID_W, (row + 1) * GRID_W)
            band = pl.ds(begin, WIN_ROWS * GRID_W)
            score = lax.dot_general(
                two_heads(q_buf[mine_rows, at]), k_buf[band, at], contract,
                preferred_element_type=f32,
            )
            weight = jnp.exp2(score + bias_buf[pair, row]).astype(bf16)
            acc = jnp.dot(weight, v_buf[band, at2], preferred_element_type=f32)
            near[pair, mine_rows, :] += acc[:GRID_W]
            near[pair, tokens + row * GRID_W : tokens + (row + 1) * GRID_W, :] += acc[GRID_W:]

    pl.loop(0, pairs // 2)(from_window)
    for mask in via_x:
        ctx_arrival(mask, 1)
        ctx_arrival(mask ^ 2, 1)
    for mask in via_y:
        ctx_arrival(mask, 2)
        ctx_arrival(mask ^ 1, 2)
    for mask in far_masks:
        spread(ctx_x, plane_rows(mask), plane_slot(mask))
    pl.loop(pairs // 2, pairs)(from_window)

    for mask in far_masks:
        finish(ctx_x, plane_rows(mask), plane_slot(mask))
    far_rows = ctx_half(True)

    mix_slot = plane_slot(0) + size // 4

    def mix_copy(pair):
        at = pl.ds(pl.multiple_of(pair * LANES, LANES), LANES)
        return remote(
            mix.at[0, :, at], mix.at[1, :, at],
            tp_send.at[mix_slot + pair], tp_recv.at[mix_slot + pair], {"tp": other},
        )

    @pl.loop(0, pairs)
    def _(pair):
        at = pl.ds(pl.multiple_of(pair * LANES, LANES), LANES)
        acc = near[pair] + from_ctx(pair, far_rows)
        mixed = acc[:, :LANES] / acc[:, LANES:]
        left = lax.broadcasted_iota(jnp.int32, (tokens, LANES), 1) < HEAD_DIM
        mix[0, :, at] = jnp.where(left, mixed[:tokens], mixed[tokens:]).astype(bf16)
        mix_copy(pair).start()

    arrived("wo")
    out = jnp.dot(
        mix[0], wo[pl.ds(pl.multiple_of(mine * lane, lane), lane), :], preferred_element_type=f32
    )
    for pair in range(pairs):
        mix_copy(pair).wait()
    out = out + jnp.dot(
        mix[1], wo[pl.ds(pl.multiple_of(other * lane, lane), lane), :], preferred_element_type=f32
    )
    out_ref[...] = (own_x[:, cols].astype(f32) + mod[4:5, cols] * out).astype(bf16)

    for copy in started:
        copy.wait_send()

    for k in range(chunks):
        partner_copy(k).wait_send()

    @pl.when(has_ahead)
    def _():
        for k in range(chunks):
            relay_copy(k).wait_send()


def fused_body(
    latent, context, cond, cond_ctx, shift_weight, scale_weight, gate_weight, norm_gain,
    query_weight, key_weight, value_weight, query_gain, key_gain, offset_bias, out_weight,
):
    size = lax.axis_size("sp")
    total_rows = (latent.shape[0] // GRID_W) * size
    tokens, width = latent.shape
    share, lane = shift_weight.shape[1], query_weight.shape[1]
    reach = WIN_ROWS // 2
    halo = reach * GRID_W
    kv_rows = tokens + 2 * halo
    ctx_rows = context.shape[0] * size
    pairs = lane // LANES
    packed = share // 2 + share // 8
    depth = size // 4 - 1
    copies = 4 + 4 * depth
    swaps = 1 + 2 * reach + size // 4 + pairs
    bf16, f32 = jnp.bfloat16, jnp.float32
    vmem = pl.BlockSpec(memory_space=pltpu.VMEM)
    hbm = pl.BlockSpec(memory_space=pltpu.HBM)
    dma = pltpu.SemaphoreType.DMA
    return pl.pallas_call(
        functools.partial(fused_kernel, total_rows),
        out_shape=pltpu.VMEM((tokens, share), latent.dtype),
        in_specs=[hbm] * 15,
        out_specs=vmem,
        scratch_shapes=[
            pltpu.VMEM((1,) + cond.shape, bf16),
            pltpu.VMEM((1,) + cond_ctx.shape, bf16),
            pltpu.VMEM((width // LANES, LANES), bf16),
            pltpu.VMEM((1,) + query_gain.shape, bf16),
            pltpu.VMEM((1,) + key_gain.shape, bf16),
            pltpu.VMEM((offset_bias.shape[1], offset_bias.shape[0], offset_bias.shape[2]), f32),
            pltpu.VMEM((tokens, width), bf16),
            pltpu.VMEM((2, halo, width), bf16),
            pltpu.VMEM((ctx_rows, width), bf16),
            pltpu.VMEM((3,) + shift_weight.shape, bf16),
            pltpu.VMEM(query_weight.shape, bf16),
            pltpu.VMEM(key_weight.shape, bf16),
            pltpu.VMEM(value_weight.shape, bf16),
            pltpu.VMEM(out_weight.shape, bf16),
            pltpu.VMEM((8, packed), f32),
            pltpu.VMEM((3, 8, packed), f32),
            pltpu.VMEM((8, packed), f32),
            pltpu.VMEM((depth, 8, packed), f32),
            pltpu.VMEM((2, 8, packed), f32),
            pltpu.VMEM((8, width), f32),
            pltpu.VMEM((1, width), f32),
            pltpu.VMEM((tokens, lane), bf16),
            pltpu.VMEM((kv_rows, lane), bf16),
            pltpu.VMEM((kv_rows, 2 * lane), bf16),
            pltpu.VMEM((ctx_rows, lane), bf16),
            pltpu.VMEM((ctx_rows, 2 * lane), bf16),
            pltpu.VMEM((2 * WIN_ROWS, offset_bias.shape[0], LANES), f32),
            pltpu.VMEM((pairs, tokens // GRID_W, LANES, WIN_ROWS * GRID_W), f32),
            pltpu.VMEM((pairs, 2 * tokens, LANES), f32),
            pltpu.VMEM((pairs, 2 * tokens, 2 * LANES), f32),
            pltpu.VMEM((2, tokens, lane), bf16),
            dma((15,)),
            dma((3,)), dma((3,)),
            dma((depth,)), dma((depth,)),
            dma((copies,)), dma((copies,)),
            dma((reach,)), dma((reach,)),
            dma((reach,)), dma((reach,)),
            dma((swaps,)), dma((swaps,)),
        ],
        compiler_params=pltpu.CompilerParams(collective_id=0, has_side_effects=True),
        name="fused",
    )(
        latent, context, cond[None, :], cond_ctx[None, :],
        shift_weight, scale_weight, gate_weight,
        norm_gain.reshape(width // LANES, LANES),
        query_weight, key_weight, value_weight,
        query_gain[None, :], key_gain[None, :],
        jnp.transpose(offset_bias, (1, 0, 2)),
        out_weight,
    )


def choose(latent, context, *rest):
    rows_dev = latent.shape[0] // GRID_W
    lane = rest[6].shape[1]
    size = lax.axis_size("sp")
    fits = size >= 4 and size & (size - 1) == 0 and context.shape[0] % 8 == 0
    aligned = lane % LANES == 0 and 2 * GRID_W == LANES
    if fits and aligned and lax.axis_size("tp") == 2 and rows_dev == WIN_ROWS // 2:
        return fused_body(latent, context, *rest)
    if fits and aligned and rows_dev >= WIN_ROWS // 2:
        return fast_body(latent, context, *rest)
    return body(latent, context, *rest)


def solution(mesh):
    in_specs = (
        P("sp", None),
        P("sp", None),
        P("sp"),
        P("sp"),
        P("sp", "tp"),
        P("sp", "tp"),
        P("sp", "tp"),
        P(),
        P(None, "tp"),
        P(None, "tp"),
        P(None, "tp"),
        P(),
        P(),
        P("tp", None, None),
        P(None, "tp"),
    )
    out_specs = P("sp", "tp")
    return jax.shard_map(choose, mesh=mesh, in_specs=in_specs, out_specs=out_specs, check_vma=False)
```

```python
import functools

import jax
import jax.numpy as jnp
import numpy as np
from jax import lax
from jax.experimental import pallas as pl
from jax.experimental.pallas import tpu as pltpu
from jax.sharding import PartitionSpec as P

HEAD_DIM = 64
WIN_ROWS = 8
WIN_COLS = 16
GRID_W = 64


EPS = 1e-06


def padded_2(block, sides, width):
    for axis, dim in sides:
        count = lax.axis_size(axis)
        forward = [(i, i + 1) for i in range(count - 1)]
        backward = [(target, source) for source, target in forward]
        low = lax.ppermute(
            lax.slice_in_dim(block, block.shape[dim] - width, None, axis=dim), axis, forward
        )
        high = lax.ppermute(lax.slice_in_dim(block, 0, width, axis=dim), axis, backward)
        block = jnp.concatenate([low, block, high], axis=dim)
    return block


def modulate(rows, norm_gain, scale, shift):
    values = rows.astype(jnp.float32)
    normed = values * lax.rsqrt(jnp.mean(values * values, axis=-1, keepdims=True) + EPS)
    return (normed * norm_gain.astype(jnp.float32) * (1.0 + scale) + shift).astype(jnp.bfloat16)


def project_heads(hidden, weight, gain):
    raw = jnp.dot(hidden, weight, preferred_element_type=jnp.float32)
    split = raw.reshape(hidden.shape[0], -1, HEAD_DIM)
    if gain is None:
        return split.astype(jnp.bfloat16)
    normed = split * lax.rsqrt(jnp.mean(split * split, axis=-1, keepdims=True) + EPS)
    return (normed * gain.astype(jnp.float32)).astype(jnp.bfloat16)


def body(
    latent,
    context,
    cond,
    cond_ctx,
    shift_weight,
    scale_weight,
    gate_weight,
    norm_gain,
    query_weight,
    key_weight,
    value_weight,
    query_gain,
    key_gain,
    offset_bias,
    out_weight,
):
    width = latent.shape[1]
    col_width = shift_weight.shape[1]
    tp_offset = lax.axis_index("tp") * col_width
    act = jax.nn.silu(cond.astype(jnp.float32)).astype(jnp.bfloat16)
    act_ctx = jax.nn.silu(cond_ctx.astype(jnp.float32)).astype(jnp.bfloat16)
    acts = jnp.stack([act, act_ctx])
    terms = jnp.concatenate(
        [
            jnp.dot(acts, shift_weight, preferred_element_type=jnp.float32),
            jnp.dot(acts, scale_weight, preferred_element_type=jnp.float32),
            jnp.dot(acts[:1], gate_weight, preferred_element_type=jnp.float32),
        ],
        axis=0,
    )
    placed = lax.dynamic_update_slice_in_dim(
        jnp.zeros((5, width), jnp.float32), terms, tp_offset, 1
    )
    full = lax.psum(placed, ("sp", "tp"))
    shift, shift_ctx, scale, scale_ctx, gate = (full[0], full[1], full[2], full[3], full[4])
    heads_dev = offset_bias.shape[0]
    lane = heads_dev * HEAD_DIM
    all_rows = lax.all_gather(context, "sp", axis=0, tiled=True)
    hidden_ctx = modulate(all_rows, norm_gain, scale_ctx, shift_ctx)
    ctx_keys = project_heads(hidden_ctx, key_weight, key_gain)
    ctx_values = project_heads(hidden_ctx, value_weight, None)
    hidden = modulate(latent, norm_gain, scale, shift)
    queries = project_heads(hidden, query_weight, query_gain)
    keys = project_heads(hidden, key_weight, key_gain)
    values = project_heads(hidden, value_weight, None)
    rows_dev = latent.shape[0] // GRID_W
    reach = WIN_ROWS // 2
    grid_kv = jnp.stack(
        [keys.reshape(rows_dev, GRID_W, lane), values.reshape(rows_dev, GRID_W, lane)], axis=1
    )
    padded = padded_2(grid_kv, (("sp", 0),), reach)
    total_rows = rows_dev * lax.axis_size("sp")
    base = lax.axis_index("sp") * rows_dev
    local_rows = base + jnp.arange(rows_dev, dtype=jnp.int32)
    first = jnp.clip(local_rows - reach, 0, total_rows - WIN_ROWS)
    window_rows = jnp.arange(WIN_ROWS, dtype=jnp.int32)
    band_index = (first - base + reach)[:, None] + window_rows[None, :]
    band = jnp.take(padded, band_index, axis=0)
    n_blocks = GRID_W // WIN_COLS
    span = 2 * WIN_COLS
    starts = [
        min(max(block * WIN_COLS - WIN_COLS // 2, 0), GRID_W - span) for block in range(n_blocks)
    ]
    blocked = jnp.stack([band[:, :, :, begin : begin + span] for begin in starts], axis=3)
    blocked = blocked.reshape(rows_dev, WIN_ROWS, 2, n_blocks, span, heads_dev, HEAD_DIM)
    key_blocks = blocked[:, :, 0]
    value_blocks = blocked[:, :, 1]
    query_col = np.arange(n_blocks)[:, None, None] * WIN_COLS + np.arange(WIN_COLS)[None, :, None]
    key_col = np.array(starts)[:, None, None] + np.arange(span)[None, None, :]
    window_first = np.clip(query_col - WIN_COLS // 2, 0, GRID_W - WIN_COLS)
    inside = (key_col >= window_first) & (key_col < window_first + WIN_COLS)
    col_offset = np.clip(key_col - query_col + WIN_COLS - 1, 0, 2 * WIN_COLS - 2)
    col_onehot = (col_offset[..., None] == np.arange(2 * WIN_COLS - 1)).astype(np.float32)
    row_offset = first[:, None] + window_rows[None, :] - local_rows[:, None] + WIN_ROWS - 1
    row_onehot = (row_offset[..., None] == jnp.arange(2 * WIN_ROWS - 1, dtype=jnp.int32)).astype(
        jnp.float32
    )
    by_col = jnp.einsum(
        "hxc,bqkc->hxbqk", offset_bias, jnp.asarray(col_onehot), precision=lax.Precision.HIGHEST
    )
    bias = jnp.einsum("rjx,hxbqk->rhbqjk", row_onehot, by_col, precision=lax.Precision.HIGHEST)
    factor = HEAD_DIM ** (-0.5)
    grid_q = queries.reshape(rows_dev, n_blocks, WIN_COLS, heads_dev, HEAD_DIM)
    local_scores = (
        jnp.einsum("rbqhd,rjbkhd->rhbqjk", grid_q, key_blocks, preferred_element_type=jnp.float32)
        * factor
    )
    local_scores = jnp.where(jnp.asarray(inside)[:, :, None, :], local_scores + bias, -jnp.inf)
    band_len = WIN_ROWS * span
    local_scores = local_scores.reshape(rows_dev, heads_dev, n_blocks, WIN_COLS, band_len)
    ctx_scores = (
        jnp.einsum("rbqhd,chd->rhbqc", grid_q, ctx_keys, preferred_element_type=jnp.float32)
        * factor
    )
    scores = jnp.concatenate([local_scores, ctx_scores], axis=-1)
    top = jnp.max(scores, axis=-1, keepdims=True)
    expd = jnp.exp(scores - top)
    weights = (expd / jnp.sum(expd, axis=-1, keepdims=True)).astype(jnp.bfloat16)
    local_w = weights[..., :band_len].reshape(
        rows_dev, heads_dev, n_blocks, WIN_COLS, WIN_ROWS, span
    )
    mixed = jnp.einsum(
        "rhbqjk,rjbkhd->rbqhd", local_w, value_blocks, preferred_element_type=jnp.float32
    )
    mixed = mixed + jnp.einsum(
        "rhbqc,chd->rbqhd", weights[..., band_len:], ctx_values, preferred_element_type=jnp.float32
    )
    mixed = mixed.astype(jnp.bfloat16).reshape(latent.shape[0], lane)
    projected = jnp.dot(
        lax.all_gather(mixed, "tp", axis=1, tiled=True),
        out_weight,
        preferred_element_type=jnp.float32,
    )
    own_cols = lax.dynamic_slice_in_dim(latent, tp_offset, col_width, 1).astype(jnp.float32)
    gate_cols = lax.dynamic_slice_in_dim(gate, tp_offset, col_width, 0)
    return (own_cols + gate_cols[None, :] * projected).astype(jnp.bfloat16)


LANES = 128
NEG = -1e30


def head_norm(raw, gain, ones):
    square = raw * raw
    high = square.astype(jnp.bfloat16)
    low = (square - high.astype(jnp.float32)).astype(jnp.bfloat16)
    parts = []
    for begin in range(0, raw.shape[1], LANES):
        cut = slice(begin, begin + LANES)
        parts.append(
            jnp.dot(high[:, cut], ones, preferred_element_type=jnp.float32)
            + jnp.dot(low[:, cut], ones, preferred_element_type=jnp.float32)
        )
    mean = jnp.concatenate(parts, axis=1) * (1.0 / HEAD_DIM)
    return raw * lax.rsqrt(mean + EPS) * gain


def attend_kernel(
    total_rows,
    low_ref,
    own_ref,
    high_ref,
    ctx_ref,
    mod_ref,
    norm_gain_ref,
    wq_ref,
    wk_ref,
    wv_ref,
    query_gain_ref,
    key_gain_ref,
    table_ref,
    out_ref,
    q_buf,
    k_buf,
    v_buf,
    ck_buf,
    cv_buf,
    low_vmem,
    own_vmem,
    high_vmem,
    ctx_vmem,
    wq_vmem,
    wk_vmem,
    wv_vmem,
    sems,
):
    tokens, lane = out_ref.shape
    streams = {}
    for place, (name, source, target) in enumerate(
        (
            ("own", own_ref, own_vmem),
            ("wk", wk_ref, wk_vmem),
            ("wv", wv_ref, wv_vmem),
            ("wq", wq_ref, wq_vmem),
            ("low", low_ref, low_vmem),
            ("high", high_ref, high_vmem),
            ("ctx", ctx_ref, ctx_vmem),
        )
    ):
        streams[name] = pltpu.make_async_copy(source, target, sems.at[place])
        streams[name].start()
    rows_dev = tokens // GRID_W
    reach = WIN_ROWS // 2
    halo = reach * GRID_W
    heads = lane // HEAD_DIM
    norm_gain = norm_gain_ref[...].astype(jnp.float32)
    half = lax.broadcasted_iota(jnp.int32, (LANES, LANES), 0) // HEAD_DIM
    half_t = lax.broadcasted_iota(jnp.int32, (LANES, LANES), 1) // HEAD_DIM
    ones = (half == half_t).astype(jnp.float32).astype(jnp.bfloat16)
    query_gain = jnp.concatenate([query_gain_ref[...].astype(jnp.float32)] * heads, axis=1)
    key_gain = jnp.concatenate([key_gain_ref[...].astype(jnp.float32)] * heads, axis=1)

    def hidden_of(x, shift, scale):
        values = x.astype(jnp.float32)
        inv = lax.rsqrt(jnp.mean(values * values, axis=-1, keepdims=True) + EPS)
        return (values * inv * (norm_gain * (1.0 + scale)) + shift).astype(jnp.bfloat16)

    def keys_values(hidden, k_out, v_out, at):
        raw = jnp.dot(hidden, wk_vmem[...], preferred_element_type=jnp.float32)
        k_out[pl.ds(at, hidden.shape[0]), :] = head_norm(raw, key_gain, ones).astype(jnp.bfloat16)
        v_out[pl.ds(at, hidden.shape[0]), :] = jnp.dot(
            hidden, wv_vmem[...], preferred_element_type=jnp.float32
        ).astype(jnp.bfloat16)

    shift, shift_ctx = mod_ref[0:1, :], mod_ref[1:2, :]
    scale, scale_ctx = mod_ref[2:3, :], mod_ref[3:4, :]
    step = min(256, tokens)
    streams["own"].wait()
    for begin in range(0, tokens, step):
        hidden = hidden_of(own_vmem[begin : begin + step, :], shift, scale)
        if begin == 0:
            streams["wk"].wait()
            streams["wv"].wait()
        keys_values(hidden, k_buf, v_buf, halo + begin)
        if begin == 0:
            streams["wq"].wait()
        raw = jnp.dot(hidden, wq_vmem[...], preferred_element_type=jnp.float32)
        q_buf[begin : begin + step, :] = (
            head_norm(raw, query_gain, ones).astype(jnp.bfloat16) * HEAD_DIM ** (-0.5)
        ).astype(jnp.bfloat16)
    streams["low"].wait()
    keys_values(hidden_of(low_vmem[...], shift, scale), k_buf, v_buf, 0)
    streams["high"].wait()
    keys_values(hidden_of(high_vmem[...], shift, scale), k_buf, v_buf, halo + tokens)
    ctx_step = min(256, ctx_vmem.shape[0])
    streams["ctx"].wait()

    @pl.loop(0, ctx_vmem.shape[0] // ctx_step)
    def _(block):
        at = pl.multiple_of(block * ctx_step, ctx_step)
        hidden = hidden_of(ctx_vmem[pl.ds(at, ctx_step), :], shift_ctx, scale_ctx)
        keys_values(hidden, ck_buf, cv_buf, at)

    base = lax.axis_index("sp") * rows_dev
    query_col = lax.broadcasted_iota(jnp.int32, (GRID_W, LANES), 0)
    lane_at = lax.broadcasted_iota(jnp.int32, (GRID_W, LANES), 1)
    key_col = lane_at % GRID_W
    window_first = jnp.clip(query_col - WIN_COLS // 2, 0, GRID_W - WIN_COLS)
    inside = (key_col >= window_first) & (key_col < window_first + WIN_COLS)
    first_head = lane_at < HEAD_DIM
    per_tile = LANES // GRID_W
    contract = (((1,), (1,)), ((), ()))

    @pl.loop(0, lane // LANES)
    def _(pair):
        cols = pl.ds(pl.multiple_of(pair * LANES, LANES), LANES)
        for row in range(rows_dev):
            first = jnp.clip(base + row - reach, 0, total_rows - WIN_ROWS)
            begin = pl.multiple_of((first - base + reach) * GRID_W, GRID_W)
            offset = first - base - row + WIN_ROWS - 1
            mine = slice(row * GRID_W, (row + 1) * GRID_W)
            query = q_buf[mine, cols]
            zero = jnp.zeros_like(query)
            query2 = jnp.concatenate(
                [jnp.where(first_head, query, zero), jnp.where(first_head, zero, query)], axis=0
            )
            band = pl.ds(begin, WIN_ROWS * GRID_W)
            local = lax.dot_general(
                query2, k_buf[band, cols], contract, preferred_element_type=jnp.float32
            )
            ctx = lax.dot_general(
                query2, ck_buf[:, cols], contract, preferred_element_type=jnp.float32
            )
            biases = []
            for head in range(2):
                tiles = []
                for tile in range(WIN_ROWS // per_tile):
                    entry = (pair * 2 + head) * (2 * WIN_ROWS) + offset + tile * per_tile
                    line = jnp.broadcast_to(table_ref[entry], (GRID_W, LANES))
                    moved = pltpu.roll(line, LANES - (WIN_COLS - 1), 1, stride=1, stride_axis=0)
                    tiles.append(jnp.where(inside, moved, NEG))
                biases.append(jnp.concatenate(tiles, axis=1))
            local = local + jnp.concatenate(biases, axis=0)
            top = jnp.maximum(
                jnp.max(local, axis=-1, keepdims=True), jnp.max(ctx, axis=-1, keepdims=True)
            )
            local = jnp.exp(local - top)
            ctx = jnp.exp(ctx - top)
            total = jnp.sum(local, axis=-1, keepdims=True) + jnp.sum(ctx, axis=-1, keepdims=True)
            mixed = jnp.dot(
                local.astype(jnp.bfloat16), v_buf[band, cols], preferred_element_type=jnp.float32
            ) + jnp.dot(
                ctx.astype(jnp.bfloat16), cv_buf[:, cols], preferred_element_type=jnp.float32
            )
            mixed = mixed / total
            out_ref[mine, cols] = jnp.where(
                first_head, mixed[:GRID_W], mixed[GRID_W:]
            ).astype(jnp.bfloat16)


def bias_lines(offset_bias):
    heads = offset_bias.shape[0]
    wide = jnp.pad(offset_bias, ((0, 0), (0, 2), (0, GRID_W - offset_bias.shape[2])))
    lines = jnp.concatenate([wide[:, :-1], wide[:, 1:]], axis=2)
    return lines.reshape(heads * 2 * WIN_ROWS, 1, LANES)


def attend(
    low, own, high, ctx, mod, norm_gain, wq, wk, wv, query_gain, key_gain, offset_bias, total_rows
):
    tokens, lane = own.shape[0], wq.shape[1]
    halo = low.shape[0]
    rows = tokens + 2 * halo
    vmem = pl.BlockSpec(memory_space=pltpu.VMEM)
    hbm = pl.BlockSpec(memory_space=pl.ANY)
    return pl.pallas_call(
        functools.partial(attend_kernel, total_rows),
        out_shape=jax.ShapeDtypeStruct((tokens, lane), jnp.bfloat16),
        in_specs=[hbm] * 4 + [vmem] * 2 + [hbm] * 3 + [vmem] * 3,
        out_specs=vmem,
        scratch_shapes=[
            pltpu.VMEM((tokens, lane), jnp.bfloat16),
            pltpu.VMEM((rows, lane), jnp.bfloat16),
            pltpu.VMEM((rows, lane), jnp.bfloat16),
            pltpu.VMEM((ctx.shape[0], lane), jnp.bfloat16),
            pltpu.VMEM((ctx.shape[0], lane), jnp.bfloat16),
        ]
        + [pltpu.VMEM(x.shape, x.dtype) for x in (low, own, high, ctx, wq, wk, wv)]
        + [pltpu.SemaphoreType.DMA((7,))],
        cost_estimate=pl.CostEstimate(
            flops=12 * tokens * own.shape[1] * lane, bytes_accessed=1 << 24, transcendentals=1 << 21
        ),
        name="attend",
    )(
        low, own, high, ctx, mod,
        norm_gain[None, :],
        wq, wk, wv,
        query_gain[None, :],
        key_gain[None, :],
        bias_lines(offset_bias),
    )


def bit_flip(index, bit):
    return index + bit - 2 * bit * ((index // bit) % 2)


def exchange_kernel(
    bits,
    tp_size,
    cond_ref,
    cond_ctx_ref,
    shift_ref,
    scale_ref,
    gate_ref,
    latent_ref,
    context_ref,
    mod_ref,
    low_ref,
    high_ref,
    ctx_ref,
    sums,
    arrived,
    local_sem,
    mod_send,
    mod_recv,
    ctx_send,
    ctx_recv,
    halo_send,
    halo_recv,
    tp_send,
    tp_recv,
):
    me = lax.axis_index("sp")
    mine = lax.axis_index("tp")
    size = lax.axis_size("sp")
    mesh_ids = pl.DeviceIdType.MESH
    barrier = pltpu.get_barrier_semaphore()
    for bit in bits:
        pl.semaphore_signal(
            barrier, inc=1, device_id={"sp": bit_flip(me, bit)}, device_id_type=mesh_ids
        )
    for away in range(1, tp_size):
        pl.semaphore_signal(
            barrier, inc=1, device_id={"tp": (mine + away) % tp_size}, device_id_type=mesh_ids
        )

    for away in (1, size - 1):
        pl.semaphore_signal(
            barrier, inc=1, device_id={"sp": (me + away) % size}, device_id_type=mesh_ids
        )

    share = latent_ref.shape[1] // tp_size
    cols = pl.ds(pl.multiple_of(mine * share, share), share)
    block = context_ref.shape[0]

    def rows_of(mask):
        index = me
        for bit in bits:
            if mask & bit:
                index = bit_flip(index, bit)
        return pl.ds(pl.multiple_of(index * block, block), block)

    keep = pltpu.make_async_copy(
        context_ref.at[:, cols], ctx_ref.at[rows_of(0), cols], local_sem.at[0]
    )
    keep.start()

    def silu(ref):
        v = ref[...].astype(jnp.float32)
        return (v / (1.0 + jnp.exp(-v))).astype(jnp.bfloat16)

    acts = jnp.concatenate([silu(cond_ref), silu(cond_ctx_ref)], axis=0)
    f32 = jnp.float32
    sums[0, 0:2, :] = jnp.dot(acts, shift_ref[...], preferred_element_type=f32)
    sums[0, 2:4, :] = jnp.dot(acts, scale_ref[...], preferred_element_type=f32)
    sums[0, 4:5, :] = jnp.dot(acts, gate_ref[...], preferred_element_type=f32)[0:1]

    pl.semaphore_wait(barrier, len(bits) + tp_size + 1)

    def remote(source, target, send, recv, where):
        return pltpu.make_async_remote_copy(
            src_ref=source, dst_ref=target, send_sem=send, recv_sem=recv,
            device_id=where, device_id_type=mesh_ids,
        )

    tokens = latent_ref.shape[0]
    halo = low_ref.shape[0]
    up = remote(
        latent_ref.at[pl.ds(tokens - halo, halo), cols], low_ref.at[:, cols],
        halo_send.at[0], halo_recv.at[0], {"sp": me + 1},
    )
    down = remote(
        latent_ref.at[pl.ds(0, halo), cols], high_ref.at[:, cols],
        halo_send.at[1], halo_recv.at[1], {"sp": me - 1},
    )
    keep.wait()
    held = [0]
    pending = {}
    started = []
    count = 0
    for step, bit in enumerate(bits):
        where = {"sp": bit_flip(me, bit)}
        term = remote(
            sums.at[step], arrived.at[step], mod_send.at[step], mod_recv.at[step], where
        )
        term.start()
        for mask in list(held):
            if mask in pending:
                pending.pop(mask).wait_recv()
            place = ctx_ref.at[rows_of(mask), cols]
            copy = remote(place, place, ctx_send.at[count], ctx_recv.at[count], where)
            copy.start()
            started.append(copy)
            pending[mask | bit] = remote(
                ctx_ref.at[rows_of(mask | bit), cols], ctx_ref.at[rows_of(mask | bit), cols],
                ctx_send.at[count], ctx_recv.at[count], where,
            )
            held.append(mask | bit)
            count += 1
        if step == 0:

            @pl.when(me < size - 1)
            def _():
                up.start()

            @pl.when(me > 0)
            def _():
                down.start()

        term.wait()
        sums[step + 1] = sums[step] + arrived[step]

    width = sums.shape[2]
    own = pl.ds(pl.multiple_of(mine * width, width), width)
    mod_ref[:, own] = sums[len(bits)]

    def spread(place, slot):
        copies = []
        for away in range(1, tp_size):
            at = slot * (tp_size - 1) + away - 1
            copies.append(
                remote(
                    place, place, tp_send.at[at], tp_recv.at[at], {"tp": (mine + away) % tp_size}
                )
            )
        for copy in copies:
            copy.start()

    def finish(ref, span, slot):
        for away in range(1, tp_size):
            at = slot * (tp_size - 1) + away - 1
            source = (mine + tp_size - away) % tp_size
            came = ref.at[:, pl.ds(pl.multiple_of(source * span, span), span)]
            wait = remote(came, came, tp_send.at[at], tp_recv.at[at], {"tp": source})
            wait.wait_send()
            wait.wait_recv()

    spread(mod_ref.at[:, own], 0)

    @pl.when(me > 0)
    def _():
        up.wait_recv()
        spread(low_ref.at[:, cols], 1)

    @pl.when(me < size - 1)
    def _():
        down.wait_recv()
        spread(high_ref.at[:, cols], 2)

    for mask in list(pending):
        pending.pop(mask).wait_recv()
    spread(ctx_ref.at[:, cols], 3)
    for copy in started:
        copy.wait_send()

    @pl.when(me < size - 1)
    def _():
        up.wait_send()

    @pl.when(me > 0)
    def _():
        down.wait_send()

    finish(mod_ref, width, 0)

    @pl.when(me > 0)
    def _():
        finish(low_ref, share, 1)

    @pl.when(me < size - 1)
    def _():
        finish(high_ref, share, 2)

    finish(ctx_ref, share, 3)


def doubling_order(size):
    bits = [1 << k for k in range(size.bit_length() - 1)]
    return tuple(bits[:1] + bits[:0:-1])


def exchange(latent, context, cond, cond_ctx, shift_weight, scale_weight, gate_weight):
    size, tp_size = lax.axis_size("sp"), lax.axis_size("tp")
    bits = doubling_order(size)
    width = latent.shape[1]
    col_width = shift_weight.shape[1]
    halo = WIN_ROWS // 2 * GRID_W
    vmem = pl.BlockSpec(memory_space=pltpu.VMEM)
    hbm = pl.BlockSpec(memory_space=pl.ANY)
    dma = pltpu.SemaphoreType.DMA
    tp_copies = max(4 * (tp_size - 1), 1)
    f32 = jnp.float32
    return pl.pallas_call(
        functools.partial(exchange_kernel, bits, tp_size),
        out_shape=[
            jax.ShapeDtypeStruct((5, width), f32),
            jax.ShapeDtypeStruct((halo, width), latent.dtype),
            jax.ShapeDtypeStruct((halo, width), latent.dtype),
            jax.ShapeDtypeStruct((context.shape[0] * size, width), context.dtype),
        ],
        in_specs=[vmem] * 5 + [hbm] * 2,
        out_specs=[vmem] * 4,
        scratch_shapes=[
            pltpu.VMEM((len(bits) + 1, 5, col_width), f32),
            pltpu.VMEM((len(bits), 5, col_width), f32),
            dma((1,)),
            dma((len(bits),)),
            dma((len(bits),)),
            dma((size,)),
            dma((size,)),
            dma((2,)),
            dma((2,)),
            dma((tp_copies,)),
            dma((tp_copies,)),
        ],
        compiler_params=pltpu.CompilerParams(collective_id=0, has_side_effects=True),
        name="exchange",
    )(cond[None, :], cond_ctx[None, :], shift_weight, scale_weight, gate_weight, latent, context)


def fast_body(
    latent, context, cond, cond_ctx, shift_weight, scale_weight, gate_weight, norm_gain,
    query_weight, key_weight, value_weight, query_gain, key_gain, offset_bias, out_weight,
):
    col_width = shift_weight.shape[1]
    tp_offset = lax.axis_index("tp") * col_width
    mod, low, high, all_ctx = exchange(
        latent, context, cond, cond_ctx, shift_weight, scale_weight, gate_weight
    )
    total_rows = (latent.shape[0] // GRID_W) * lax.axis_size("sp")
    mixed = attend(
        low, latent, high, all_ctx, mod, norm_gain, query_weight, key_weight, value_weight,
        query_gain, key_gain, offset_bias, total_rows,
    )
    projected = jnp.dot(
        lax.all_gather(mixed, "tp", axis=1, tiled=True),
        out_weight,
        preferred_element_type=jnp.float32,
    )
    own_cols = lax.dynamic_slice_in_dim(latent, tp_offset, col_width, 1).astype(jnp.float32)
    gate_cols = lax.dynamic_slice_in_dim(mod[4], tp_offset, col_width, 0)
    return (own_cols + gate_cols[None, :] * projected).astype(jnp.bfloat16)


LOG2E = 1.4426950408889634


def fused_kernel(
    total_rows,
    latent_ref, context_ref, cond_hbm, cond_ctx_hbm, shift_ref, scale_ref, gate_ref,
    norm_gain_hbm, wq_ref, wk_ref, wv_ref, query_gain_hbm, key_gain_hbm, table_hbm, wo_ref,
    out_ref,
    cond_ref, cond_ctx_ref, norm_gain_ref, query_gain_ref, key_gain_ref, table_ref,
    own_x, halo_x, ctx_x, ws, wq, wk, wv, wo,
    sums, plane_in, sums_z, z_in, final, mod, gain_row,
    q_buf, k_buf, v_buf, ck_buf, cv_buf, lines, bias_buf, bound_buf, near, mix,
    local_sem, plane_send, plane_recv, z_send, z_recv, ctx_send, ctx_recv,
    halo_send, halo_recv, relay_send, relay_recv, tp_send, tp_recv,
):
    f32, bf16 = jnp.float32, jnp.bfloat16
    me, mine = lax.axis_index("sp"), lax.axis_index("tp")
    size = lax.axis_size("sp")
    other = 1 - mine
    mesh_ids = pl.DeviceIdType.MESH
    tokens, width = own_x.shape
    block = context_ref.shape[0]
    share = width // 2
    lane = wq.shape[1]
    pairs = lane // LANES
    rows_dev = tokens // GRID_W
    reach = WIN_ROWS // 2
    halo = reach * GRID_W
    half_ctx = ctx_x.shape[0] // 2
    cols = pl.ds(pl.multiple_of(mine * share, share), share)

    def flip(mask):
        index = me
        bit = 1
        while bit < size:
            if mask & bit:
                index = bit_flip(index, bit)
            bit *= 2
        return index

    def remote(source, target, send, recv, where):
        return pltpu.make_async_remote_copy(
            src_ref=source, dst_ref=target, send_sem=send, recv_sem=recv,
            device_id=where, device_id_type=mesh_ids,
        )

    plane = [1, 2, 3]
    depth = [4 * k for k in sorted(range(1, size // 4), key=lambda k: (k.bit_count(), k))]

    streams = {}
    for place, (name, source, target) in enumerate(
        (
            ("cond", cond_hbm, cond_ref),
            ("cond_ctx", cond_ctx_hbm, cond_ctx_ref),
            ("shift", shift_ref, ws.at[0]),
            ("scale", scale_ref, ws.at[1]),
            ("gate", gate_ref, ws.at[2]),
            ("keep", context_ref.at[:, cols],
             ctx_x.at[pl.ds(pl.multiple_of(me * block, block), block), cols]),
            ("table", table_hbm, table_ref),
            ("norm_gain", norm_gain_hbm, norm_gain_ref),
            ("query_gain", query_gain_hbm, query_gain_ref),
            ("key_gain", key_gain_hbm, key_gain_ref),
            ("own", latent_ref, own_x),
            ("wk", wk_ref, wk),
            ("wv", wv_ref, wv),
            ("wq", wq_ref, wq),
            ("wo", wo_ref, wo),
        )
    ):
        streams[name] = pltpu.make_async_copy(source, target, local_sem.at[place])

    def fetch(*names):
        for name in names:
            streams[name].start()

    def arrived(*names):
        for name in names:
            streams[name].wait()

    fetch("cond", "cond_ctx", "shift", "scale", "gate", "keep", "table")
    fetch("norm_gain", "query_gain", "key_gain")

    barrier = pltpu.get_barrier_semaphore()
    for mask in plane + depth:
        pl.semaphore_signal(
            barrier, inc=1, device_id={"sp": flip(mask)}, device_id_type=mesh_ids
        )
    pl.semaphore_signal(barrier, inc=1, device_id={"tp": other}, device_id_type=mesh_ids)
    parity = me % 2
    ahead = me + 2 - 4 * parity
    behind = me - 2 + 4 * parity
    pl.semaphore_signal(
        barrier, inc=1, device_id={"sp": (ahead + size) % size}, device_id_type=mesh_ids
    )
    pl.semaphore_signal(
        barrier, inc=1, device_id={"sp": (behind + size) % size}, device_id_type=mesh_ids
    )

    def silu(ref):
        v = ref[...].astype(f32)
        return (v / (1.0 + jnp.exp(-v))).astype(bf16)

    arrived("cond", "cond_ctx", "shift", "scale", "gate")
    fetch("own", "wk", "wv", "wq", "wo")
    acts = jnp.concatenate([silu(cond_ref), silu(cond_ctx_ref)], axis=0)
    part = share // 2
    for place in range(2):
        raw = jnp.dot(acts, ws[place], preferred_element_type=f32)
        sums[2 * place : 2 * place + 2, 0:part] = raw[:, :part]
        sums[4 + 2 * place : 6 + 2 * place, 0:part] = raw[:, part:]
    raw = jnp.dot(acts, ws[2], preferred_element_type=f32)
    piece = share // 8
    for k in range(8):
        sums[k : k + 1, part : part + piece] = raw[0:1, k * piece : (k + 1) * piece]

    arrived("keep", "table", "norm_gain", "query_gain", "key_gain")
    norm_gain = norm_gain_ref[...].astype(f32)
    for k in range(width // LANES):
        gain_row[0:1, k * LANES : (k + 1) * LANES] = norm_gain[k : k + 1, :]
    offsets = table_ref.shape[0]
    span = table_ref.shape[2]
    lines[...] = jnp.zeros_like(lines)
    for k in range(offsets):
        lines[k, :, 0:span] = table_ref[k]
    for k in range(offsets):
        lines[k] = lines[k] + pltpu.roll(lines[k + 1], GRID_W, 1)
    for p in range(pairs):
        filled = jnp.ones((v_buf.shape[0], LANES), bf16)
        v_buf[:, (2 * p + 1) * LANES : (2 * p + 2) * LANES] = filled
        cv_buf[:, (2 * p + 1) * LANES : (2 * p + 2) * LANES] = filled[: cv_buf.shape[0]]

    base = me * rows_dev
    query_col = lax.broadcasted_iota(jnp.int32, (GRID_W, LANES), 0)
    lane_at = lax.broadcasted_iota(jnp.int32, (GRID_W, LANES), 1)
    key_col = lane_at % GRID_W
    window_first = jnp.clip(query_col - WIN_COLS // 2, 0, GRID_W - WIN_COLS)
    inside = (key_col >= window_first) & (key_col < window_first + WIN_COLS)
    per_tile = LANES // GRID_W
    tiles_row = WIN_ROWS // per_tile

    def bias_of(pair):
        for head in range(2):
            for row in range(rows_dev):
                first = jnp.clip(base + row - reach, 0, total_rows - WIN_ROWS)
                offset = first - base - row + WIN_ROWS - 1
                tiles = []
                for tile in range(tiles_row):
                    line = jnp.broadcast_to(
                        lines[offset + tile * per_tile, pl.ds(pair * 2 + head, 1), :],
                        (GRID_W, LANES),
                    )
                    moved = pltpu.roll(line, LANES - (WIN_COLS - 1), 1, stride=1, stride_axis=0)
                    tiles.append(jnp.where(inside, moved, NEG))
                top = tiles[0]
                for tile in tiles[1:]:
                    top = jnp.maximum(top, tile)
                bound = jnp.maximum(jnp.max(top, axis=-1, keepdims=True), 0.0)
                at = pl.ds(head * GRID_W, GRID_W)
                for tile in range(tiles_row):
                    bias_buf[pair, row, at, tile * LANES : (tile + 1) * LANES] = (
                        tiles[tile] - bound
                    ) * LOG2E
                bound_buf[pair, pl.ds(head * tokens + row * GRID_W, GRID_W), :] = jnp.broadcast_to(
                    bound * LOG2E, (GRID_W, LANES)
                )

    early = pairs // 2
    pl.semaphore_wait(barrier, len(plane) + len(depth) + 3)

    first_stage = []
    for place, mask in enumerate(plane):
        copy = remote(
            sums, plane_in.at[place], plane_send.at[place], plane_recv.at[place],
            {"sp": flip(mask)},
        )
        copy.start()
        first_stage.append(copy)

    slots = {}

    def ctx_copy(mask, toward):
        slot = slots.setdefault((mask, toward), len(slots))
        rows = pl.ds(pl.multiple_of(flip(mask) * block, block), block)
        place = ctx_x.at[rows, cols]
        return remote(
            place, place, ctx_send.at[slot], ctx_recv.at[slot], {"sp": flip(toward)}
        )

    def ctx_arrival(mask, toward):
        slot = slots[(mask, toward)]
        rows = pl.ds(pl.multiple_of(flip(mask ^ toward) * block, block), block)
        place = ctx_x.at[rows, cols]
        remote(place, place, ctx_send.at[slot], ctx_recv.at[slot], {"sp": flip(toward)}).wait_recv()

    started = []

    def ctx_start(mask, toward):
        copy = ctx_copy(mask, toward)
        copy.start()
        started.append(copy)

    ctx_start(0, 1)
    ctx_start(0, 2)

    chunks = reach
    step = halo // chunks

    def partner_copy(k):
        rows = pl.ds(k * step, step)
        return remote(
            latent_ref.at[rows, cols], halo_x.at[parity, rows, cols],
            halo_send.at[k], halo_recv.at[k], {"sp": flip(1)},
        )

    def relay_copy(k):
        rows = pl.ds(k * step, step)
        return remote(
            halo_x.at[1 - parity, rows, cols], halo_x.at[parity, rows, cols],
            relay_send.at[k], relay_recv.at[k], {"sp": ahead},
        )

    has_ahead = jnp.logical_and(ahead >= 0, ahead < size)
    has_behind = jnp.logical_and(behind >= 0, behind < size)

    def spread(ref, rows, slot):
        remote(
            ref.at[rows, cols], ref.at[rows, cols], tp_send.at[slot], tp_recv.at[slot],
            {"tp": other},
        ).start()

    def finish(ref, rows, slot):
        theirs = pl.ds(pl.multiple_of(other * share, share), share)
        copy = remote(
            ref.at[rows, theirs], ref.at[rows, theirs], tp_send.at[slot], tp_recv.at[slot],
            {"tp": other},
        )
        copy.wait_send()
        copy.wait_recv()

    def relay(k):
        partner_copy(k).wait_recv()

        @pl.when(has_ahead)
        def _():
            relay_copy(k).start()

        spread(halo_x.at[1 - parity], pl.ds(k * step, step), 1 + k)

    def plane_rows(mask):
        return pl.ds(pl.multiple_of(flip(mask) // 4 * 4 * block, 4 * block), 4 * block)

    def plane_slot(mask):
        return 1 + 2 * chunks + mask // 4

    near_masks = [mask for mask in depth if mask < size // 2]
    far_masks = [mask for mask in depth if mask >= size // 2][::-1]
    partner_copy(0).start()
    for mask in near_masks:
        ctx_start(0, mask)

    pl.loop(0, early)(bias_of)
    for copy in first_stage:
        copy.wait()
    total = sums[...]
    for place in range(len(plane)):
        total = total + plane_in[place]
    sums_z[...] = total
    second_stage = []
    for place, mask in enumerate(depth):
        copy = remote(
            sums_z, z_in.at[place], z_send.at[place], z_recv.at[place], {"sp": flip(mask)}
        )
        copy.start()
        second_stage.append(copy)
    for mask in far_masks:
        ctx_start(0, mask)
    ctx_arrival(0, 1)
    ctx_start(1, 2)
    for mask in near_masks:
        ctx_arrival(0, mask)
        ctx_start(mask, 1)
        ctx_start(mask, 2)
    for k in range(1, chunks):
        partner_copy(k).start()

    pl.loop(early, pairs)(bias_of)
    for copy in second_stage:
        copy.wait()
    total = sums_z[...]
    for place in range(len(depth)):
        total = total + z_in[place]
    final[0] = total
    swap = remote(final.at[0], final.at[1], tp_send.at[0], tp_recv.at[0], {"tp": other})
    swap.start()
    relay(0)
    ctx_arrival(0, 2)
    ctx_arrival(1, 2)
    spread(ctx_x, plane_rows(0), plane_slot(0))
    for mask in near_masks:
        ctx_arrival(mask, 1)
        ctx_start(mask ^ 1, 2)
    swap.wait()
    for side in range(2):
        came = final[side]
        at = pl.multiple_of((mine if side == 0 else other) * share, share)
        mod[0:4, pl.ds(at, part)] = came[0:4, 0:part]
        mod[0:4, pl.ds(at + part, part)] = came[4:8, 0:part]
        for k in range(8):
            mod[4:5, pl.ds(at + k * piece, piece)] = came[k : k + 1, part : part + piece]

    norm = gain_row[...]
    wide = 2 * LANES
    half_r = lax.broadcasted_iota(jnp.int32, (wide, wide), 0) // HEAD_DIM
    half_c = lax.broadcasted_iota(jnp.int32, (wide, wide), 1) // HEAD_DIM
    ones = (half_r == half_c).astype(f32).astype(bf16)
    heads = lane // HEAD_DIM
    query_gain = jnp.concatenate(
        [query_gain_ref[...].astype(f32) * (HEAD_DIM ** (-0.5) * LOG2E)] * heads, axis=1
    )
    key_gain = jnp.concatenate([key_gain_ref[...].astype(f32)] * heads, axis=1)

    def normed(raw, gain):
        square = (raw * raw).astype(bf16)
        parts = [
            jnp.dot(square[:, begin : begin + wide], ones, preferred_element_type=f32)
            for begin in range(0, lane, wide)
        ]
        mean = jnp.concatenate(parts, axis=1) * (1.0 / HEAD_DIM)
        return (raw * lax.rsqrt(mean + EPS) * gain).astype(bf16)

    def hidden_of(x, shift, scale):
        values = x.astype(f32)
        inv = lax.rsqrt(jnp.mean(values * values, axis=-1, keepdims=True) + EPS)
        return (values * inv * (norm * (1.0 + scale)) + shift).astype(bf16)

    def keys_values(hidden, k_out, v_out, at, between=None):
        count = hidden.shape[0]
        raw = jnp.dot(hidden, wk[...], preferred_element_type=f32)
        k_out[pl.ds(at, count), :] = normed(raw, key_gain)
        if between is not None:
            between()
        raw = jnp.dot(hidden, wv[...], preferred_element_type=f32).astype(bf16)
        for p in range(pairs):
            v_out[pl.ds(at, count), 2 * p * LANES : (2 * p + 1) * LANES] = raw[
                :, p * LANES : (p + 1) * LANES
            ]

    shift, shift_ctx = mod[0:1, :], mod[1:2, :]
    scale, scale_ctx = mod[2:3, :], mod[3:4, :]
    arrived("own", "wk", "wv", "wq")
    hidden = hidden_of(own_x[...], shift, scale)
    keys_values(hidden, k_buf, v_buf, halo)
    relay(1)
    q_buf[...] = normed(jnp.dot(hidden, wq[...], preferred_element_type=f32), query_gain)

    for mask in near_masks:
        ctx_arrival(mask, 2)
        ctx_arrival(mask ^ 1, 2)
        spread(ctx_x, plane_rows(mask), plane_slot(mask))
    relay(2)
    for mask in [0] + near_masks:
        finish(ctx_x, plane_rows(mask), plane_slot(mask))

    def far_on():
        for mask in far_masks:
            ctx_arrival(0, mask)
            ctx_start(mask, 1)

    def ctx_half(far):
        top = size // 2
        index = me // top
        if far:
            index = 1 - index
        at = pl.multiple_of(index * half_ctx, half_ctx)
        hidden = hidden_of(ctx_x[pl.ds(at, half_ctx), :], shift_ctx, scale_ctx)
        keys_values(hidden, ck_buf, cv_buf, at, None if far else far_on)
        return pl.ds(at, half_ctx)

    near_rows = ctx_half(False)
    for k in range(3, chunks):
        relay(k)
    for mask in far_masks:
        ctx_start(mask, 2)

    contract = (((1,), (1,)), ((), ()))

    def two_heads(query):
        zero = jnp.zeros_like(query)
        left = lax.broadcasted_iota(jnp.int32, query.shape, 1) < HEAD_DIM
        return jnp.concatenate(
            [jnp.where(left, query, zero), jnp.where(left, zero, query)], axis=0
        )

    def from_ctx(pair, rows):
        at = pl.ds(pl.multiple_of(pair * LANES, LANES), LANES)
        at2 = pl.ds(pl.multiple_of(pair * 2 * LANES, 2 * LANES), 2 * LANES)
        score = lax.dot_general(
            two_heads(q_buf[:, at]), ck_buf[rows, at], contract, preferred_element_type=f32
        )
        shown = jnp.concatenate([bound_buf[pair]] * (half_ctx // LANES), axis=1)
        weight = jnp.exp2(score - shown).astype(bf16)
        return jnp.dot(weight, cv_buf[rows, at2], preferred_element_type=f32)

    for pair in range(pairs):
        near[pair] = from_ctx(pair, near_rows)

    for k in range(chunks):
        finish(halo_x.at[1 - parity], pl.ds(k * step, step), 1 + k)
    stride = halo + tokens
    keys_values(
        hidden_of(halo_x[1 - parity], shift, scale),
        k_buf, v_buf, pl.multiple_of((1 - parity) * stride, stride),
    )
    for mask in far_masks:
        ctx_arrival(mask, 1)
        ctx_start(mask ^ 1, 2)

    @pl.when(has_behind)
    def _():
        for k in range(chunks):
            relay_copy(k).wait_recv()
            spread(halo_x.at[parity], pl.ds(k * step, step), 1 + chunks + k)

    @pl.when(has_behind)
    def _():
        for k in range(chunks):
            finish(halo_x.at[parity], pl.ds(k * step, step), 1 + chunks + k)

    keys_values(
        hidden_of(halo_x[parity], shift, scale),
        k_buf, v_buf, pl.multiple_of(parity * stride, stride),
    )

    def from_window(pair):
        at = pl.ds(pl.multiple_of(pair * LANES, LANES), LANES)
        at2 = pl.ds(pl.multiple_of(pair * 2 * LANES, 2 * LANES), 2 * LANES)
        for row in range(rows_dev):
            first = jnp.clip(base + row - reach, 0, total_rows - WIN_ROWS)
            begin = pl.multiple_of((first - base + reach) * GRID_W, GRID_W)
            mine_rows = slice(row * GRID_W, (row + 1) * GRID_W)
            band = pl.ds(begin, WIN_ROWS * GRID_W)
            score = lax.dot_general(
                two_heads(q_buf[mine_rows, at]), k_buf[band, at], contract,
                preferred_element_type=f32,
            )
            weight = jnp.exp2(score + bias_buf[pair, row]).astype(bf16)
            acc = jnp.dot(weight, v_buf[band, at2], preferred_element_type=f32)
            near[pair, mine_rows, :] += acc[:GRID_W]
            near[pair, tokens + row * GRID_W : tokens + (row + 1) * GRID_W, :] += acc[GRID_W:]

    pl.loop(0, pairs // 2)(from_window)
    for mask in far_masks:
        ctx_arrival(mask, 2)
        ctx_arrival(mask ^ 1, 2)
    for mask in far_masks:
        spread(ctx_x, plane_rows(mask), plane_slot(mask))
    pl.loop(pairs // 2, pairs)(from_window)

    for mask in far_masks:
        finish(ctx_x, plane_rows(mask), plane_slot(mask))
    far_rows = ctx_half(True)

    mix_slot = plane_slot(0) + size // 4

    def mix_copy(pair):
        at = pl.ds(pl.multiple_of(pair * LANES, LANES), LANES)
        return remote(
            mix.at[0, :, at], mix.at[1, :, at],
            tp_send.at[mix_slot + pair], tp_recv.at[mix_slot + pair], {"tp": other},
        )

    for pair in range(pairs):
        at = slice(pair * LANES, (pair + 1) * LANES)
        acc = near[pair] + from_ctx(pair, far_rows)
        mixed = acc[:, :LANES] / acc[:, LANES:]
        left = lax.broadcasted_iota(jnp.int32, (tokens, LANES), 1) < HEAD_DIM
        mix[0, :, at] = jnp.where(left, mixed[:tokens], mixed[tokens:]).astype(bf16)
        mix_copy(pair).start()

    arrived("wo")
    out = jnp.dot(
        mix[0], wo[pl.ds(pl.multiple_of(mine * lane, lane), lane), :], preferred_element_type=f32
    )
    begin = pl.multiple_of(other * lane, lane)
    most = lane - LANES
    for pair in range(pairs - 1):
        mix_copy(pair).wait()
    out = out + jnp.dot(
        mix[1, :, :most], wo[pl.ds(begin, most), :], preferred_element_type=f32
    )
    mix_copy(pairs - 1).wait()
    out = out + jnp.dot(
        mix[1, :, most:], wo[pl.ds(begin + most, LANES), :], preferred_element_type=f32
    )
    out_ref[...] = (own_x[:, cols].astype(f32) + mod[4:5, cols] * out).astype(bf16)

    for copy in started:
        copy.wait_send()

    for k in range(chunks):
        partner_copy(k).wait_send()

    @pl.when(has_ahead)
    def _():
        for k in range(chunks):
            relay_copy(k).wait_send()


def fused_body(
    latent, context, cond, cond_ctx, shift_weight, scale_weight, gate_weight, norm_gain,
    query_weight, key_weight, value_weight, query_gain, key_gain, offset_bias, out_weight,
):
    size = lax.axis_size("sp")
    total_rows = (latent.shape[0] // GRID_W) * size
    tokens, width = latent.shape
    share, lane = shift_weight.shape[1], query_weight.shape[1]
    reach = WIN_ROWS // 2
    halo = reach * GRID_W
    kv_rows = tokens + 2 * halo
    ctx_rows = context.shape[0] * size
    pairs = lane // LANES
    packed = share // 2 + share // 8
    depth = size // 4 - 1
    copies = 4 + 4 * depth
    swaps = 1 + 2 * reach + size // 4 + pairs
    bf16, f32 = jnp.bfloat16, jnp.float32
    vmem = pl.BlockSpec(memory_space=pltpu.VMEM)
    hbm = pl.BlockSpec(memory_space=pltpu.HBM)
    dma = pltpu.SemaphoreType.DMA
    return pl.pallas_call(
        functools.partial(fused_kernel, total_rows),
        out_shape=pltpu.VMEM((tokens, share), latent.dtype),
        in_specs=[hbm] * 15,
        out_specs=vmem,
        scratch_shapes=[
            pltpu.VMEM((1,) + cond.shape, bf16),
            pltpu.VMEM((1,) + cond_ctx.shape, bf16),
            pltpu.VMEM((width // LANES, LANES), bf16),
            pltpu.VMEM((1,) + query_gain.shape, bf16),
            pltpu.VMEM((1,) + key_gain.shape, bf16),
            pltpu.VMEM((offset_bias.shape[1], offset_bias.shape[0], offset_bias.shape[2]), f32),
            pltpu.VMEM((tokens, width), bf16),
            pltpu.VMEM((2, halo, width), bf16),
            pltpu.VMEM((ctx_rows, width), bf16),
            pltpu.VMEM((3,) + shift_weight.shape, bf16),
            pltpu.VMEM(query_weight.shape, bf16),
            pltpu.VMEM(key_weight.shape, bf16),
            pltpu.VMEM(value_weight.shape, bf16),
            pltpu.VMEM(out_weight.shape, bf16),
            pltpu.VMEM((8, packed), f32),
            pltpu.VMEM((3, 8, packed), f32),
            pltpu.VMEM((8, packed), f32),
            pltpu.VMEM((depth, 8, packed), f32),
            pltpu.VMEM((2, 8, packed), f32),
            pltpu.VMEM((8, width), f32),
            pltpu.VMEM((1, width), f32),
            pltpu.VMEM((tokens, lane), bf16),
            pltpu.VMEM((kv_rows, lane), bf16),
            pltpu.VMEM((kv_rows, 2 * lane), bf16),
            pltpu.VMEM((ctx_rows, lane), bf16),
            pltpu.VMEM((ctx_rows, 2 * lane), bf16),
            pltpu.VMEM((2 * WIN_ROWS, offset_bias.shape[0], LANES), f32),
            pltpu.VMEM((pairs, tokens // GRID_W, LANES, WIN_ROWS * GRID_W), f32),
            pltpu.VMEM((pairs, 2 * tokens, LANES), f32),
            pltpu.VMEM((pairs, 2 * tokens, 2 * LANES), f32),
            pltpu.VMEM((2, tokens, lane), bf16),
            dma((15,)),
            dma((3,)), dma((3,)),
            dma((depth,)), dma((depth,)),
            dma((copies,)), dma((copies,)),
            dma((reach,)), dma((reach,)),
            dma((reach,)), dma((reach,)),
            dma((swaps,)), dma((swaps,)),
        ],
        compiler_params=pltpu.CompilerParams(collective_id=0, has_side_effects=True),
        name="fused",
    )(
        latent, context, cond[None, :], cond_ctx[None, :],
        shift_weight, scale_weight, gate_weight,
        norm_gain.reshape(width // LANES, LANES),
        query_weight, key_weight, value_weight,
        query_gain[None, :], key_gain[None, :],
        jnp.transpose(offset_bias, (1, 0, 2)),
        out_weight,
    )


def choose(latent, context, *rest):
    rows_dev = latent.shape[0] // GRID_W
    lane = rest[6].shape[1]
    size = lax.axis_size("sp")
    fits = size >= 4 and size & (size - 1) == 0 and context.shape[0] % 8 == 0
    aligned = lane % LANES == 0 and 2 * GRID_W == LANES
    if fits and aligned and lax.axis_size("tp") == 2 and rows_dev == WIN_ROWS // 2:
        return fused_body(latent, context, *rest)
    if fits and aligned and rows_dev >= WIN_ROWS // 2:
        return fast_body(latent, context, *rest)
    return body(latent, context, *rest)


def solution(mesh):
    in_specs = (
        P("sp", None),
        P("sp", None),
        P("sp"),
        P("sp"),
        P("sp", "tp"),
        P("sp", "tp"),
        P("sp", "tp"),
        P(),
        P(None, "tp"),
        P(None, "tp"),
        P(None, "tp"),
        P(),
        P(),
        P("tp", None, None),
        P(None, "tp"),
    )
    out_specs = P("sp", "tp")
    return jax.shard_map(choose, mesh=mesh, in_specs=in_specs, out_specs=out_specs, check_vma=False)
```
